512 devices in a mesh: fs: 64 (over z, y), tp: 8 (over x, core).
Axes of the slice: x: 4, y: 8, z: 8, core: 2. Of those that a mesh axis runs over, the one named last changes fastest.
Arguments:
- tokens: bfloat16 [65536, 2048], P(('fs', 'tp')), may hold values from -8 to 8
- pre_mix_gain: float32 [2048], replicated, may hold values from 0.1 to 1.9
- post_mix_gain: float32 [2048], replicated, may hold values from 0.1 to 1.9
- pre_ffn_gain: float32 [2048], replicated, may hold values from 0.1 to 1.9
- post_ffn_gain: float32 [2048], replicated, may hold values from 0.1 to 1.9
- w_branch: bfloat16 [2048, 1024], P('fs', 'tp'), may hold values from -0.125 to 0.125
- w_gelu: bfloat16 [2048, 1024], P('fs', 'tp'), may hold values from -0.125 to 0.125
- conv_weight: bfloat16 [4, 1024], P(None, 'tp'), may hold values from -3 to 3
- w_rec: bfloat16 [2, 8, 128, 128], P(None, 'tp'), may hold values from -0.5 to 0.5
- w_inp: bfloat16 [2, 8, 128, 128], P(None, 'tp'), may hold values from -0.5 to 0.5
- decay: float32 [2, 1024], P(None, 'tp'), may hold values from 3 to 10
- out_weight_t: bfloat16 [2048, 1024], P('fs', 'tp'), may hold values from -0.1875 to 0.1875
- w_gate: bfloat16 [2048, 3072], P('fs', 'tp'), may hold values from -0.125 to 0.125
- w_up: bfloat16 [2048, 3072], P('fs', 'tp'), may hold values from -0.125 to 0.125
- down_weight_t: bfloat16 [2048, 3072], P('fs', 'tp'), may hold values from -0.109375 to 0.109375
Outputs:
- layer_out: bfloat16 [65536, 2048], P(('fs', 'tp'))
The draws below stay inside these ranges and needn't reach their ends.
All inputs are finite; a program needn't handle non-finite values.
Results may differ from the reference program's by a relative error of at most 0.014.
Values may be sent and summed in bfloat16 or wider, within the bound.
A program may use at most 64 MiB of HBM per device.

```python
import math
import jax
import jax.numpy as jnp
from jax import lax

D = 2048
BLOCKS = 8
BW = 128
FF = 3072
SEQ_LEN = 1024
D_LRU = 1024
TOKENS = 65536
N_FS = 64
N_TP = 8


def draw_tokens(key, part):
    noise_key = jax.random.fold_in(key, 11)
    common_key = jax.random.fold_in(key, 12)
    block_count = (TOKENS + 15) // 16
    block_index = jnp.arange(TOKENS) // 16
    common = jax.random.normal(common_key, (block_count, D), jnp.float32)
    noise = jax.random.normal(noise_key, (TOKENS, D), jnp.float32)
    values = noise + 1.2 * common[block_index]
    return jnp.clip(values, -8.0, 8.0).astype(jnp.bfloat16)


def draw_decay(key, part):
    choose_key = jax.random.fold_in(key, 21)
    slow_key = jax.random.fold_in(key, 22)
    fast_key = jax.random.fold_in(key, 23)
    fast_share = 0.5
    fast = jax.random.uniform(choose_key, (2, D_LRU), jnp.float32) < fast_share
    slow_rate = jnp.exp(jax.random.uniform(slow_key, (2, D_LRU), jnp.float32, math.log(0.3), math.log(1.5))) / SEQ_LEN
    fast_rate = 1.0 / jnp.exp(jax.random.uniform(fast_key, (2, D_LRU), jnp.float32, math.log(15.0), math.log(50.0)))
    per_step = jnp.where(fast, fast_rate, slow_rate)
    return (-jnp.log(jnp.expm1(per_step / 4.0))).astype(jnp.float32)


def steps_of(rng, shape, cuts, smallest, high):
    level, own = 1.0, jax.random.fold_in(rng, 6)
    for dim, blocks in cuts:
        steps = jnp.exp(jax.random.uniform(jax.random.fold_in(own, dim), (blocks,), jnp.float32, smallest / len(cuts), high / len(cuts)))
        level = level * jnp.repeat(steps, shape[dim] // blocks).reshape([-1 if axis == dim else 1 for axis in range(len(shape))])
    return level


def gaussian(own_key, dims, deviation, reach, split=(), held_as=jnp.bfloat16):
    values = deviation * jax.random.normal(own_key, dims, jnp.float32)
    if split:
        values = values * steps_of(own_key, dims, split, -0.22, 0.18)
    return jnp.clip(values, -reach, reach).astype(held_as)


def setup_inputs(seed: int = 0) -> dict:
    key_list = jax.random.split(jax.random.key(seed), 16)
    return {
        "tokens": draw_tokens(jax.random.fold_in(key_list[15], 71), 0),
        "pre_mix_gain": jnp.clip(1.0 + 0.18 * jax.random.normal(key_list[1], (D,), jnp.float32), 0.1, 1.9),
        "post_mix_gain": jnp.clip(1.0 + 0.18 * jax.random.normal(key_list[2], (D,), jnp.float32), 0.1, 1.9),
        "pre_ffn_gain": jnp.clip(1.0 + 0.18 * jax.random.normal(key_list[3], (D,), jnp.float32), 0.1, 1.9),
        "post_ffn_gain": jnp.clip(1.0 + 0.18 * jax.random.normal(key_list[4], (D,), jnp.float32), 0.1, 1.9),
        "w_branch": gaussian(key_list[5], (D, D_LRU), D ** -0.5, 0.125, ((0, 64), (1, 8))),
        "w_gelu": gaussian(key_list[6], (D, D_LRU), D ** -0.5, 0.125, ((0, 64), (1, 8))),
        "conv_weight": gaussian(key_list[7], (4, D_LRU), 0.5, 3.0, ((1, 8),)),
        "w_rec": gaussian(key_list[8], (2, BLOCKS, BW, BW), BW ** -0.5, 0.5, ((1, 8),)),
        "w_inp": gaussian(key_list[9], (2, BLOCKS, BW, BW), BW ** -0.5, 0.5, ((1, 8),)),
        "decay": draw_decay(jax.random.fold_in(key_list[15], 71), 0),
        "out_weight_t": gaussian(key_list[11], (D, D_LRU), D_LRU ** -0.5, 0.1875, ((0, 64), (1, 8))),
        "w_gate": gaussian(key_list[12], (D, FF), D ** -0.5, 0.125, ((0, 64), (1, 8))),
        "w_up": gaussian(key_list[13], (D, FF), D ** -0.5, 0.125, ((0, 64), (1, 8))),
        "down_weight_t": gaussian(key_list[14], (D, FF), FF ** -0.5, 0.109375, ((0, 64), (1, 8))),
    }


EPS = 1e-06

def normed(values, gain):
    factor = lax.rsqrt(lax.optimization_barrier(jnp.mean(values * values, axis=-1, keepdims=True)) + EPS)
    return values * factor * gain

def conv_short(branch, conv_weight):
    length = branch.shape[0]
    padded = jnp.pad(branch.astype(jnp.float32), ((2, 1), (0, 0)))
    weights = conv_weight.astype(jnp.float32)
    summed = weights[0] * padded[0:length]
    for offset in range(1, 4):
        summed = summed + weights[offset] * padded[offset:offset + length]
    return summed.astype(jnp.bfloat16)

def combine(earlier, later):
    return (earlier[0] * later[0], later[0] * earlier[1] + later[1])

def recurrence(conv_out, w_rec, w_inp, decay):
    length, channels = conv_out.shape
    blocks = w_rec.shape[0]
    grouped = conv_out.astype(jnp.float32).reshape(length, blocks, channels // blocks)
    rate_gate = jax.nn.sigmoid(jnp.einsum('lnc,ncd->lnd', grouped, w_rec.astype(jnp.float32)).reshape(length, channels))
    inflow = jax.nn.sigmoid(jnp.einsum('lnc,ncd->lnd', grouped, w_inp.astype(jnp.float32)).reshape(length, channels))
    log_retain = -8.0 * rate_gate * jax.nn.softplus(-decay)
    retain = jnp.exp(log_retain)
    feed = jnp.sqrt(-jnp.expm1(2.0 * log_retain)) * inflow * conv_out.astype(jnp.float32)
    unused_decay, states = lax.associative_scan(combine, (retain, feed), axis=0)
    return states

def grouped_sum(hidden, weight_t):
    group_cols = hidden.shape[1] // N_TP

    def add_group(index, summed):
        first_col = (index * group_cols).astype(jnp.int32)
        part_rows = lax.dynamic_slice_in_dim(hidden, first_col, group_cols, 1)
        part_cols = lax.dynamic_slice_in_dim(weight_t, first_col, group_cols, 1)
        partial_value = lax.dot_general(part_rows, part_cols, (((1,), (1,)), ((), ())), preferred_element_type=jnp.float32)
        rounded = lax.optimization_barrier(partial_value.astype(jnp.bfloat16))
        return summed + rounded.astype(jnp.float32)
    zero_block = jnp.zeros((hidden.shape[0], weight_t.shape[0]), jnp.float32)
    return lax.fori_loop(0, N_TP, add_group, zero_block)

def reference(tokens, pre_mix_gain, post_mix_gain, pre_ffn_gain, post_ffn_gain, w_branch, w_gelu, conv_weight, w_rec, w_inp, decay, out_weight_t, w_gate, w_up, down_weight_t):

    def one_sequence(seq_tokens):
        stream = seq_tokens.astype(jnp.float32)
        normed_in = normed(stream, pre_mix_gain).astype(jnp.bfloat16)
        branch_in = jnp.dot(normed_in, w_branch, preferred_element_type=jnp.float32).astype(jnp.bfloat16)
        gelu_in = jnp.dot(normed_in, w_gelu, preferred_element_type=jnp.float32).astype(jnp.bfloat16)
        conv_out = conv_short(branch_in, conv_weight)
        forward = recurrence(conv_out, w_rec[0], w_inp[0], decay[0])
        backward = jnp.flip(recurrence(jnp.flip(conv_out, 0), w_rec[1], w_inp[1], decay[1]), 0)
        mixer_hidden = (jax.nn.gelu(gelu_in.astype(jnp.float32)) * (forward + backward)).astype(jnp.bfloat16)
        mixer_sum = lax.dot_general(mixer_hidden, out_weight_t, (((1,), (1,)), ((), ())), preferred_element_type=jnp.float32)
        residual = (stream + normed(mixer_sum, post_mix_gain)).astype(jnp.bfloat16)
        middle = residual.astype(jnp.float32)
        normed_mid = normed(middle, pre_ffn_gain).astype(jnp.bfloat16)
        gate_proj = jnp.dot(normed_mid, w_gate, preferred_element_type=jnp.float32)
        up_proj = jnp.dot(normed_mid, w_up, preferred_element_type=jnp.float32)
        ffn_hidden = (jax.nn.silu(gate_proj) * up_proj).astype(jnp.bfloat16)
        ffn_sum = grouped_sum(ffn_hidden, down_weight_t)
        return (middle + normed(ffn_sum, post_ffn_gain)).astype(jnp.bfloat16)
    sequences = tokens.reshape(N_FS, SEQ_LEN, D)
    outputs = lax.map(one_sequence, sequences)
    return outputs.reshape(N_FS * SEQ_LEN, D)
```

```python
import jax
import jax.numpy as jnp
from jax import lax
from jax.experimental import pallas as pl
from jax.experimental.pallas import tpu as pltpu
from jax.sharding import PartitionSpec as P

EPS = 1e-06
MESH = pl.DeviceIdType.MESH
F32 = jnp.float32
BF16 = jnp.bfloat16
RING = 8
CHIPS = 4
ROWS = 128
SUB = 32
SUBS = ROWS // SUB
D = 2048
SEG = 136
NT = (((1,), (1,)), ((), ()))


def rem(a, n):
    return lax.rem(a, jnp.int32(n))


def hold(ref, sem):
    pltpu.make_async_copy(ref, ref, sem).wait()


def normed(values, gain):
    factor = lax.rsqrt(jnp.mean(values * values, axis=-1, keepdims=True) + EPS)
    return values * factor * gain


def sigmoid(v):
    return 1.0 / (1.0 + jnp.exp(-v))


def gelu(v):
    return 0.5 * v * (1.0 + jnp.tanh(0.7978845608028654 * (v + 0.044715 * v * v * v)))


def loop(count, body):
    def step(i, carry):
        body(i)
        return carry

    lax.fori_loop(0, count, step, 0)


def layer(
    tokens,
    pre_mix,
    post_mix,
    pre_ffn,
    post_ffn,
    w_branch,
    w_gelu,
    conv_weight,
    w_rec,
    w_inp,
    decay,
    out_w,
    w_gate,
    w_up,
    w_down,
    out,
    tok,
    n1,
    n2,
    a_all,
    o_all,
    f_all,
    o_own,
    branch,
    gel,
    ret0,
    ret1,
    fee0,
    fee1,
    gates,
    scale,
    carry_in,
    mixed,
    hidden,
    msum,
    res,
    gu,
    hid,
    keep,
    give,
    got,
    sums,
    land,
    load_sem,
    a_recv,
    o_recv,
    f_recv,
    ring_send,
    pre_recv,
    pre_send,
    swap_recv,
    swap_send,
    n1_recv,
    n2_recv,
    n_send,
    mix_recv,
    mix_send,
    pair_recv,
    pair_send,
    land_recv,
    land_send,
):
    f = lax.axis_index("fs")
    t = lax.axis_index("tp")
    z, y = lax.div(f, jnp.int32(RING)), rem(f, RING)
    x, c = lax.div(t, jnp.int32(2)), rem(t, 2)
    p, q = y + c * (z - y), z + c * (y - z)
    step_p, step_q = 1 + (RING - 1) * c, RING - (RING - 1) * c
    turn = 1 - 2 * c
    partner = 2 * x + 1 - c

    def place(pp, qq):
        return pp * step_p + qq * step_q

    def remote(src, dst, send, recv, fs=None, tp=None):
        return pltpu.make_async_remote_copy(
            src_ref=src,
            dst_ref=dst,
            send_sem=send,
            recv_sem=recv,
            device_id={"fs": f if fs is None else fs, "tp": t if tp is None else tp},
            device_id_type=MESH,
        )

    def chip(away):
        return rem(x + away + CHIPS, CHIPS)

    loads = [
        (w_branch, a_all.at[f, :, pl.ds(0, 128)]),
        (w_gelu, a_all.at[f, :, pl.ds(128, 128)]),
        (out_w, o_own),
        (tokens, tok),
        (w_gate, f_all.at[f, :, pl.ds(0, 384)]),
        (w_up, f_all.at[f, :, pl.ds(384, 384)]),
        (w_down, f_all.at[f, :, pl.ds(768, 384)]),
    ]
    loads = [pltpu.make_async_copy(s, d, load_sem.at[i]) for i, (s, d) in enumerate(loads)]
    for copy in loads:
        copy.start()

    barrier = pltpu.get_barrier_semaphore()

    def greet(fs, tp):
        pl.semaphore_signal(barrier, inc=1, device_id={"fs": fs, "tp": tp}, device_id_type=MESH)

    for e in range(1, RING):
        greet(place(rem(p + e, RING), q), t)
    for e in (1, RING - 1):
        greet(place(p, rem(q + e, RING)), t)
    for e in range(1, 8):
        greet(f, rem(t + e, 8))
    pl.semaphore_wait(barrier, 16)

    class Gather:
        def __init__(self, piece, recv, send):
            self.piece, self.recv, self.send = piece, recv, send

        def spread(self):
            def body(e):
                j = e + 1
                off = lax.div(j + 1, jnp.int32(2)) * (2 * rem(j, 2) - 1)
                there = place(rem(p + off + RING, RING), q)
                remote(self.piece(f), self.piece(f), self.send, self.recv.at[f], fs=there).start()

            loop(RING - 1, body)

        def slot(self, j, away):
            off = lax.div(j + 1, jnp.int32(2)) * (2 * rem(j, 2) - 1)
            return place(rem(p + off + RING, RING), rem(q + away + RING, RING))

        def pass_on(self, slot, way):
            there = place(p, rem(q + way + RING, RING))
            remote(
                self.piece(slot), self.piece(slot), self.send, self.recv.at[slot], fs=there
            ).start()

        def arrive(self, slot):
            hold(self.piece(slot), self.recv.at[slot])

        def first(self, half):
            def body(i):
                j = i + 4 * half
                slot = self.slot(j, 0)

                @pl.when(j > 0)
                def _():
                    self.arrive(slot)

                self.pass_on(slot, 1)
                self.pass_on(slot, -1)

            loop(4, body)

        def hop(self, far, half):
            def body(i):
                j = i + 4 * half
                k = j + 4 if far == 3 else j
                from_left, from_right = self.slot(j, -far), self.slot(k, far)
                self.arrive(from_left)
                self.pass_on(from_left, 1)
                self.arrive(from_right)
                self.pass_on(from_right, -1)

            loop(4, body)

        def finish(self):
            def body(j):
                self.arrive(self.slot(j + 4, -3))
                self.arrive(self.slot(j, 3))
                self.arrive(self.slot(j, 4))
                self.arrive(self.slot(j + 4, 4))

            loop(4, body)

    ga = Gather(lambda s: a_all.at[s], a_recv, ring_send.at[0])
    go = Gather(lambda s: o_all.at[s, c], o_recv, ring_send.at[1])
    gf = Gather(lambda s: f_all.at[s], f_recv, ring_send.at[2])

    loads[0].wait()
    loads[1].wait()
    ga.spread()

    loads[2].wait()
    own_lanes = pl.ds(pl.multiple_of(t * 128, 128), 128)
    for e in range(1, 8):
        other = rem(t + e, 8)
        half = rem(other, 2)
        remote(
            o_own.at[half], o_all.at[f, half, :, own_lanes], pre_send, pre_recv.at[t], tp=other
        ).start()
    own_out = pltpu.make_async_copy(o_own.at[c], o_all.at[f, c, :, own_lanes], load_sem.at[7])
    own_out.start()

    class Rows:
        def __init__(self, ref, recv, send):
            self.ref, self.recv, self.send = ref, recv, send

        def pass_on(self, at, tp):
            remote(self.ref.at[at], self.ref.at[at], self.send, self.recv.at[at], tp=tp).start()

        def arrive(self, at):
            hold(self.ref.at[at], self.recv.at[at])

        def own(self, k):
            at = t * SUBS + k
            self.pass_on(at, 2 * chip(turn) + c)
            self.pass_on(at, 2 * chip(-turn) + c)
            self.pass_on(at, partner)

        def behind(self, k):
            at = (2 * chip(-turn) + c) * SUBS + k
            self.arrive(at)
            self.pass_on(at, 2 * chip(turn) + c)
            self.pass_on(at, partner)

        def ahead(self, k):
            at = (2 * chip(turn) + c) * SUBS + k
            self.arrive(at)
            self.pass_on(at, partner)

        def far(self, k):
            at = (2 * chip(2) + c) * SUBS + k
            self.arrive(at)
            self.pass_on(at, partner)

        def paired(self, chip_at):
            for k in range(SUBS):
                self.arrive((2 * chip_at + 1 - c) * SUBS + k)

        def drain(self):
            hold(self.ref.at[pl.ds(0, 7 * SUBS)], self.send)

        def block(self, tp):
            rows = self.ref[pl.ds(tp * SUBS, SUBS)]
            return rows.reshape(ROWS, D)

    r1 = Rows(n1, n1_recv, n_send.at[0])
    r2 = Rows(n2, n2_recv, n_send.at[1])

    loads[3].wait()

    def norm_in(k):
        for h in range(SUB // 16):
            rows = tok[pl.ds(pl.multiple_of(k * SUB + 16 * h, 16), 16), :].astype(F32)
            n1[t * SUBS + k, pl.ds(16 * h, 16), :] = normed(rows, pre_mix[...]).astype(BF16)
        r1.own(k)

    loop(SUBS, norm_in)

    ga.first(0)
    ga.first(1)
    for d in range(2):
        gates[:, pl.ds(256 * d, 128)] = w_rec[d, 0]
        gates[:, pl.ds(256 * d + 128, 128)] = w_inp[d, 0]
    low = -decay[...]
    scale[...] = -8.0 * (jnp.maximum(low, 0.0) + jnp.log1p(jnp.exp(-jnp.abs(low))))
    branch[pl.ds(0, 8), :] = jnp.zeros((8, 128), F32)
    branch[pl.ds(1032, 8), :] = jnp.zeros((8, 128), F32)

    own_out.wait()
    for e in range(1, 8):
        other = rem(t + e, 8)
        lanes = pl.ds(pl.multiple_of(other * 128, 128), 128)
        hold(o_all.at[f, c, :, lanes], pre_recv.at[other])
    ga.hop(1, 0)
    go.spread()
    ga.hop(1, 1)
    r1.behind(0)
    r1.ahead(0)
    ga.hop(2, 0)
    ga.hop(2, 1)
    r1.behind(1)
    r1.ahead(1)
    go.first(0)
    ga.hop(3, 0)
    go.first(1)
    r1.behind(2)
    r1.ahead(2)
    loads[4].wait()
    loads[5].wait()
    loads[6].wait()
    gf.spread()
    ga.finish()
    r1.behind(3)
    r1.ahead(3)

    def project(chip_at):
        r1.paired(chip_at)
        rows = n1[pl.ds(2 * chip_at * SUBS, 2 * SUBS)].reshape(2 * ROWS, D)
        both = jnp.dot(rows, a_all[...].reshape(D, 256), preferred_element_type=F32)
        both = both.astype(BF16).astype(F32)
        at = chip_at * 2 * ROWS
        branch[pl.ds(pl.multiple_of(at + 8, 8), 2 * ROWS), :] = both[:, :128]
        gel[pl.ds(pl.multiple_of(at, 8), 2 * ROWS), :] = both[:, 128:]

    project(x)
    go.hop(1, 0)
    project(chip(turn))
    go.hop(1, 1)
    project(chip(-turn))
    go.hop(2, 0)
    for k in range(SUBS):
        r1.far(k)
    project(chip(2))

    taps = conv_weight[...].astype(F32)

    def gate(s):
        window = branch[pl.ds(pl.multiple_of(s * 128, 8), 144), :]
        summed = taps[0:1] * window[6:134]
        for offset in range(1, 4):
            summed = summed + taps[offset : offset + 1] * window[6 + offset : 134 + offset]
        conv = summed.astype(BF16)
        wide = conv.astype(F32)
        both = jnp.dot(conv, gates[...], preferred_element_type=F32)
        at = pl.ds(pl.multiple_of(s * SEG, 8), 128)
        for d, (ret, fee) in enumerate(((ret0, fee0), (ret1, fee1))):
            rate = sigmoid(both[:, 256 * d : 256 * d + 128])
            inflow = sigmoid(both[:, 256 * d + 128 : 256 * d + 256])
            log_retain = rate * scale[pl.ds(d, 1), :]
            retain = jnp.exp(log_retain)
            u = 2.0 * log_retain
            near = 1.0 + u * (0.2 * (1.0 + u * (1.0 / 6.0)))
            near = 1.0 + u * (1.0 / 3.0) * (1.0 + u * 0.25 * near)
            near = -u * (1.0 + 0.5 * u * near)
            lost = jnp.where(u > -0.25, near, 1.0 - retain * retain)
            ret[at, :] = retain
            fee[at, :] = jnp.sqrt(lost) * inflow * wide

    loop(8, gate)
    go.hop(2, 1)

    one, zero = jnp.ones((8, 128), F32), jnp.zeros((8, 128), F32)

    def scan(i, carry):
        h0, a0, h1, a1 = carry
        for k in range(8):
            up = pl.ds(i * 8 + k, 8, stride=SEG)
            down = pl.ds(127 - (i * 8 + k), 8, stride=SEG)
            r, v = ret0[up, :], fee0[up, :]
            h0 = r * h0 + v
            a0 = r * a0
            fee0[up, :] = h0
            ret0[up, :] = a0
            r, v = ret1[down, :], fee1[down, :]
            h1 = r * h1 + v
            a1 = r * a1
            fee1[down, :] = h1
            ret1[down, :] = a1
        return h0, a0, h1, a1

    h0, a0, h1, a1 = lax.fori_loop(0, 16, scan, (zero, one, zero, one))
    state = jnp.zeros((1, 128), F32)
    for s in range(8):
        carry_in[s : s + 1, :] = state
        state = a0[s : s + 1] * state + h0[s : s + 1]
    state = jnp.zeros((1, 128), F32)
    for s in reversed(range(8)):
        carry_in[8 + s : 9 + s, :] = state
        state = a1[s : s + 1] * state + h1[s : s + 1]

    def mix(e):
        s = rem(t + e, 8)
        at = pl.ds(pl.multiple_of(s * SEG, 8), 128)
        state = fee0[at, :] + ret0[at, :] * carry_in[pl.ds(s, 1), :]
        state = state + (fee1[at, :] + ret1[at, :] * carry_in[pl.ds(8 + s, 1), :])
        value = gelu(gel[pl.ds(pl.multiple_of(s * 128, 8), 128), :]) * state
        mixed[s] = value.astype(BF16)

        @pl.when(e > 0)
        def _():
            remote(mixed.at[s], hidden.at[t], mix_send, mix_recv.at[t], tp=s).start()

        @pl.when(e == 0)
        def _():
            hidden[s] = value.astype(BF16)

    loop(8, mix)
    go.hop(3, 0)
    gf.first(0)
    gf.first(1)
    go.finish()

    def swap(part):
        rows = o_all.at[pl.ds(16 * part, 16), c]
        remote(rows, rows, swap_send, swap_recv.at[part], tp=partner).start()

    loop(4, swap)
    for e in range(1, 8):
        other = rem(t + e, 8)
        hold(hidden.at[other], mix_recv.at[other])
    gf.hop(1, 0)

    wide_hidden = jnp.concatenate([hidden[i] for i in range(8)], axis=1)

    def project_out(part):
        hold(o_all.at[pl.ds(16 * part, 16), 1 - c], swap_recv.at[part])
        weight = o_all[pl.ds(16 * part, 16)].reshape(512, 1024)
        msum[:, pl.ds(pl.multiple_of(part * 512, 128), 512)] = lax.dot_general(
            wide_hidden, weight, NT, preferred_element_type=F32
        )

    loop(4, project_out)

    def norm_mid(k):
        for h in range(SUB // 16):
            at = pl.ds(pl.multiple_of(k * SUB + 16 * h, 16), 16)
            total = tok[at, :].astype(F32) + normed(msum[at, :], post_mix[...])
            total = total.astype(BF16)
            res[at, :] = total
            n2[t * SUBS + k, pl.ds(16 * h, 16), :] = normed(
                total.astype(F32), pre_ffn[...]
            ).astype(BF16)
        r2.own(k)

    loop(SUBS, norm_mid)
    gf.hop(1, 1)
    gf.hop(2, 0)
    for k in range(SUBS):
        r2.behind(k)
        r2.ahead(k)
    gf.hop(2, 1)
    gf.hop(3, 0)
    for k in range(SUBS):
        r2.far(k)
    gf.finish()

    def feed_forward(i):
        away = jnp.where(i == 0, 2, jnp.where(i == 1, -turn, jnp.where(i == 2, turn, 0)))
        there = chip(away)
        r2.paired(there)
        rows = jnp.concatenate([r2.block(2 * there + 1 - c), r2.block(2 * there + c)], axis=0)
        for n in range(3):
            gu[:, pl.ds(256 * n, 256)] = jnp.dot(
                rows, f_all[:, :, pl.ds(256 * n, 256)].reshape(D, 256), preferred_element_type=F32
            )
        for h in range(4):
            at = pl.ds(64 * h, 64)
            g = gu[at, pl.ds(0, 384)]
            hid[at, :] = (g * sigmoid(g) * gu[at, pl.ds(384, 384)]).astype(BF16)

        def down(n):
            weight = f_all[pl.ds(16 * n, 16), :, pl.ds(768, 384)].reshape(512, 384)
            part = lax.dot_general(hid[...], weight, NT, preferred_element_type=F32)
            lanes = pl.ds(pl.multiple_of(512 * n, 128), 512)
            give[i, :, lanes] = part[:ROWS].astype(BF16)
            keep[i, :, lanes] = part[ROWS:]

        loop(4, down)
        other = jnp.where(i == 1, 2, jnp.where(i == 2, 1, i))
        remote(give.at[i], got.at[other], pair_send, pair_recv.at[other], tp=partner).start()

        @pl.when(i == 1)
        def _():
            pass_sum(0)

    def pass_sum(o):
        target = 2 * chip(-turn if o == 1 else turn) + c
        hold(got.at[o], pair_recv.at[o])

        def add(k):
            if o == 2:
                hold(land.at[0, k], land_recv.at[0, k])
            for h in range(SUB // 16):
                at = pl.ds(pl.multiple_of(k * SUB + 16 * h, 16), 16)
                inner = pl.ds(16 * h, 16)
                total = keep[o, at, :] + got[o, at, :].astype(F32)
                if o == 2:
                    total = total + land[0, k, inner, :].astype(F32)
                sums[o, k, inner, :] = total.astype(BF16)
            remote(
                sums.at[o, k], land.at[o, k], land_send, land_recv.at[o, k], tp=target
            ).start()

        loop(SUBS, add)

    loop(4, feed_forward)
    pass_sum(1)
    pass_sum(2)
    hold(got.at[3], pair_recv.at[3])

    def last(k):
        hold(land.at[1, k], land_recv.at[1, k])
        hold(land.at[2, k], land_recv.at[2, k])
        for h in range(SUB // 16):
            at = pl.ds(pl.multiple_of(k * SUB + 16 * h, 16), 16)
            inner = pl.ds(16 * h, 16)
            total = keep[3, at, :] + got[3, at, :].astype(F32)
            total = total + land[1, k, inner, :].astype(F32)
            total = total + land[2, k, inner, :].astype(F32)
            final = res[at, :].astype(F32) + normed(total, post_ffn[...])
            out[at, :] = final.astype(BF16)

    loop(SUBS, last)

    hold(a_all.at[pl.ds(0, 63)], ring_send.at[0])
    hold(o_all.at[pl.ds(0, 63), 0], ring_send.at[1])
    hold(f_all.at[pl.ds(0, 63)], ring_send.at[2])
    hold(o_all.at[0, 0, :, pl.ds(0, 896)], pre_send)
    hold(o_all.at[:, c], swap_send)
    r1.drain()
    r2.drain()
    hold(mixed.at[pl.ds(0, 7)], mix_send)
    hold(give, pair_send)
    hold(sums, land_send)


def per_device(
    tokens,
    pre_mix_gain,
    post_mix_gain,
    pre_ffn_gain,
    post_ffn_gain,
    w_branch,
    w_gelu,
    conv_weight,
    w_rec,
    w_inp,
    decay,
    out_weight_t,
    w_gate,
    w_up,
    down_weight_t,
):
    gains = [
        g.reshape(1, D) for g in (pre_mix_gain, post_mix_gain, pre_ffn_gain, post_ffn_gain)
    ]
    vmem = pl.BlockSpec(memory_space=pltpu.VMEM)
    far = pl.BlockSpec(memory_space=pl.ANY)
    dma = pltpu.SemaphoreType.DMA
    return pl.pallas_call(
        layer,
        out_shape=jax.ShapeDtypeStruct((ROWS, D), BF16),
        in_specs=[far] + [vmem] * 4 + [far, far] + [vmem] * 4 + [far] * 4,
        out_specs=vmem,
        scratch_shapes=[
            pltpu.VMEM((ROWS, D), BF16),
            pltpu.VMEM((8 * SUBS, SUB, D), BF16),
            pltpu.VMEM((8 * SUBS, SUB, D), BF16),
            pltpu.VMEM((64, 32, 256), BF16),
            pltpu.VMEM((64, 2, 16, 1024), BF16),
            pltpu.VMEM((64, 32, 1152), BF16),
            pltpu.VMEM((2, 16, 128), BF16),
            pltpu.VMEM((1040, 128), F32),
            pltpu.VMEM((1024, 128), F32),
            pltpu.VMEM((8 * SEG, 128), F32),
            pltpu.VMEM((8 * SEG, 128), F32),
            pltpu.VMEM((8 * SEG, 128), F32),
            pltpu.VMEM((8 * SEG, 128), F32),
            pltpu.VMEM((128, 512), BF16),
            pltpu.VMEM((2, 128), F32),
            pltpu.VMEM((16, 128), F32),
            pltpu.VMEM((8, 128, 128), BF16),
            pltpu.VMEM((8, 128, 128), BF16),
            pltpu.VMEM((ROWS, D), F32),
            pltpu.VMEM((ROWS, D), BF16),
            pltpu.VMEM((2 * ROWS, 768), F32),
            pltpu.VMEM((2 * ROWS, 384), BF16),
            pltpu.VMEM((4, ROWS, D), F32),
            pltpu.VMEM((4, ROWS, D), BF16),
            pltpu.VMEM((4, ROWS, D), BF16),
            pltpu.VMEM((3, SUBS, SUB, D), BF16),
            pltpu.VMEM((3, SUBS, SUB, D), BF16),
            dma((8,)),
            dma((64,)),
            dma((64,)),
            dma((64,)),
            dma((3,)),
            dma((8,)),
            dma,
            dma((4,)),
            dma,
            dma((8 * SUBS,)),
            dma((8 * SUBS,)),
            dma((2,)),
            dma((8,)),
            dma,
            dma((4,)),
            dma,
            dma((3, SUBS)),
            dma,
        ],
        compiler_params=pltpu.CompilerParams(
            collective_id=0, has_side_effects=True, vmem_limit_bytes=60 * 1024 * 1024
        ),
    )(
        tokens,
        *gains,
        w_branch,
        w_gelu,
        conv_weight,
        w_rec,
        w_inp,
        decay,
        out_weight_t.reshape(2, 16, 128),
        w_gate,
        w_up,
        down_weight_t,
    )


def solution(mesh):
    return jax.shard_map(
        per_device,
        mesh=mesh,
        in_specs=(
            P(("fs", "tp"), None),
            P(),
            P(),
            P(),
            P(),
            P("fs", "tp"),
            P("fs", "tp"),
            P(None, "tp"),
            P(None, "tp", None, None),
            P(None, "tp", None, None),
            P(None, "tp"),
            P("fs", "tp"),
            P("fs", "tp"),
            P("fs", "tp"),
            P("fs", "tp"),
        ),
        out_specs=P(("fs", "tp"), None),
        check_vma=False,
    )
```

```python
import jax
import jax.numpy as jnp
from jax import lax
from jax.experimental import pallas as pl
from jax.experimental.pallas import tpu as pltpu
from jax.sharding import PartitionSpec as P

EPS = 1e-06
MESH = pl.DeviceIdType.MESH
F32 = jnp.float32
BF16 = jnp.bfloat16
RING = 8
CHIPS = 4
ROWS = 128
SUB = 32
SUBS = ROWS // SUB
D = 2048
SEG = 136
NT = (((1,), (1,)), ((), ()))


def rem(a, n):
    return lax.rem(a, jnp.int32(n))


def hold(ref, sem):
    pltpu.make_async_copy(ref, ref, sem).wait()


def normed(values, gain):
    factor = lax.rsqrt(jnp.mean(values * values, axis=-1, keepdims=True) + EPS)
    return values * factor * gain


def sigmoid(v):
    return 0.5 + 0.5 * jnp.tanh(0.5 * v)


def gelu(v):
    return 0.5 * v * (1.0 + jnp.tanh(0.7978845608028654 * (v + 0.044715 * v * v * v)))


def loop(count, body):
    def step(i, carry):
        body(i)
        return carry

    lax.fori_loop(0, count, step, 0)


def layer(
    tokens,
    pre_mix_hbm,
    post_mix_hbm,
    pre_ffn_hbm,
    post_ffn_hbm,
    w_branch,
    w_gelu,
    conv_hbm,
    w_rec_hbm,
    w_inp_hbm,
    decay_hbm,
    out_w,
    w_gate,
    w_up,
    w_down,
    out,
    pre_mix,
    post_mix,
    pre_ffn,
    post_ffn,
    conv_weight,
    w_rec,
    w_inp,
    decay,
    tok,
    n1,
    n2,
    a_all,
    o_all,
    f_all,
    o_own,
    branch,
    gel,
    ret0,
    ret1,
    fee0,
    fee1,
    gates,
    scale,
    carry_in,
    mixed,
    hidden,
    msum,
    res,
    gu,
    hid,
    keep,
    give,
    got,
    sums,
    land,
    final_rows,
    load_sem,
    a_recv,
    o_recv,
    f_recv,
    ring_send,
    pre_recv,
    pre_send,
    swap_recv,
    swap_send,
    n_recv,
    n_send,
    mix_recv,
    mix_send,
    pair_recv,
    pair_send,
    land_recv,
    land_send,
):
    f = lax.axis_index("fs")
    t = lax.axis_index("tp")
    z, y = lax.div(f, jnp.int32(RING)), rem(f, RING)
    x, c = lax.div(t, jnp.int32(2)), rem(t, 2)
    p, q = y + c * (z - y), z + c * (y - z)
    step_p, step_q = 1 + (RING - 1) * c, RING - (RING - 1) * c
    turn = 1 - 2 * c
    partner = 2 * x + 1 - c

    def place(pp, qq):
        return pp * step_p + qq * step_q

    def remote(src, dst, send, recv, fs=None, tp=None):
        return pltpu.make_async_remote_copy(
            src_ref=src,
            dst_ref=dst,
            send_sem=send,
            recv_sem=recv,
            device_id={"fs": f if fs is None else fs, "tp": t if tp is None else tp},
            device_id_type=MESH,
        )

    def chip(away):
        return rem(x + away + CHIPS, CHIPS)

    loads = [
        (w_branch, a_all.at[f, :, pl.ds(0, 128)]),
        (w_gelu, a_all.at[f, :, pl.ds(128, 128)]),
        (out_w, o_own),
        (tokens, tok),
        (w_gate, f_all.at[f, :, pl.ds(0, 384)]),
        (w_up, f_all.at[f, :, pl.ds(384, 384)]),
        (w_down, f_all.at[f, :, pl.ds(768, 384)]),
        (pre_mix_hbm, pre_mix),
        (conv_hbm, conv_weight),
        (w_rec_hbm, w_rec),
        (w_inp_hbm, w_inp),
        (decay_hbm, decay),
        (post_mix_hbm, post_mix),
        (pre_ffn_hbm, pre_ffn),
        (post_ffn_hbm, post_ffn),
    ]
    loads = [pltpu.make_async_copy(s, d, load_sem.at[i]) for i, (s, d) in enumerate(loads)]
    for copy in loads:
        copy.start()

    barrier = pltpu.get_barrier_semaphore()

    def greet(fs, tp):
        pl.semaphore_signal(barrier, inc=1, device_id={"fs": fs, "tp": tp}, device_id_type=MESH)

    for e in range(1, RING):
        greet(place(rem(p + e, RING), q), t)
    for e in (1, RING - 1):
        greet(place(p, rem(q + e, RING)), t)
    for e in range(1, 8):
        greet(f, rem(t + e, 8))
    pl.semaphore_wait(barrier, 16)

    class Gather:
        def __init__(self, piece, recv, send):
            self.piece, self.recv, self.send = piece, recv, send

        def spread(self):
            def body(e):
                j = e + 1
                off = lax.div(j + 1, jnp.int32(2)) * (2 * rem(j, 2) - 1)
                there = place(rem(p + off + RING, RING), q)
                remote(self.piece(f), self.piece(f), self.send, self.recv.at[f], fs=there).start()

            loop(RING - 1, body)

        def slot(self, j, away):
            off = lax.div(j + 1, jnp.int32(2)) * (2 * rem(j, 2) - 1)
            return place(rem(p + off + RING, RING), rem(q + away + RING, RING))

        def pass_on(self, slot, way):
            there = place(p, rem(q + way + RING, RING))
            remote(
                self.piece(slot), self.piece(slot), self.send, self.recv.at[slot], fs=there
            ).start()

        def arrive(self, slot):
            hold(self.piece(slot), self.recv.at[slot])

        def first(self, half):
            def body(i):
                j = i + 4 * half
                slot = self.slot(j, 0)

                @pl.when(j > 0)
                def _():
                    self.arrive(slot)

                self.pass_on(slot, 1)
                self.pass_on(slot, -1)

            loop(4, body)

        def spread_near(self):
            for e in (1, -1, 2, -2):
                there = place(rem(p + e + RING, RING), q)
                remote(self.piece(f), self.piece(f), self.send, self.recv.at[f], fs=there).start()

        def relay(self, slot, e):
            there = place(rem(p + e + RING, RING), q)
            remote(
                self.piece(slot), self.piece(slot), self.send, self.recv.at[slot], fs=there
            ).start()

        def near(self):
            for j, off in enumerate((0, 1, -1, 2, -2)):
                slot = place(rem(p + off + RING, RING), q)
                if j > 0:
                    self.arrive(slot)
                if j > 2:
                    way = 1 if off < 0 else -1
                    self.relay(slot, way)

                    @pl.when(rem(p, 2) == (0 if off < 0 else 1))
                    def _():
                        self.relay(slot, 2 * way)

                self.pass_on(slot, 1)
                self.pass_on(slot, -1)

        def late(self):
            for off in (3, -3, 4):
                slot = place(rem(p + off + RING, RING), q)
                self.arrive(slot)
                self.pass_on(slot, 1)
                self.pass_on(slot, -1)

        def hop(self, far, half):
            def body(i):
                j = i + 4 * half
                k = j + 4 if far == 3 else j
                from_left, from_right = self.slot(j, -far), self.slot(k, far)
                self.arrive(from_left)
                self.pass_on(from_left, 1)
                self.arrive(from_right)
                self.pass_on(from_right, -1)

            loop(4, body)

        def finish(self):
            def body(j):
                self.arrive(self.slot(j + 4, -3))
                self.arrive(self.slot(j, 3))
                self.arrive(self.slot(j, 4))
                self.arrive(self.slot(j + 4, 4))

            loop(4, body)

    ga = Gather(lambda s: a_all.at[s], a_recv, ring_send.at[0])
    go = Gather(lambda s: o_all.at[s, c], o_recv, ring_send.at[1])
    gf = Gather(lambda s: f_all.at[s], f_recv, ring_send.at[2])

    loads[0].wait()
    loads[1].wait()
    ga.spread()

    loads[2].wait()
    own_lanes = pl.ds(pl.multiple_of(t * 128, 128), 128)
    for e in range(1, 8):
        other = rem(t + e, 8)
        half = rem(other, 2)
        remote(
            o_own.at[half], o_all.at[f, half, :, own_lanes], pre_send, pre_recv.at[t], tp=other
        ).start()
    own_out = pltpu.make_async_copy(o_own.at[c], o_all.at[f, c, :, own_lanes], load_sem.at[15])
    own_out.start()

    class Rows:
        def __init__(self, ref, recv, send):
            self.ref, self.recv, self.send = ref, recv, send

        def pass_on(self, at, tp):
            remote(self.ref.at[at], self.ref.at[at], self.send, self.recv.at[at], tp=tp).start()

        def arrive(self, at):
            hold(self.ref.at[at], self.recv.at[at])

        def own(self, k):
            at = t * SUBS + k
            self.pass_on(at, 2 * chip(turn) + c)
            self.pass_on(at, 2 * chip(-turn) + c)
            self.pass_on(at, partner)

        def behind(self, k):
            at = (2 * chip(-turn) + c) * SUBS + k
            self.arrive(at)
            self.pass_on(at, 2 * chip(turn) + c)
            self.pass_on(at, partner)

        def ahead(self, k):
            at = (2 * chip(turn) + c) * SUBS + k
            self.arrive(at)
            self.pass_on(at, partner)

        def far(self, k):
            at = (2 * chip(2) + c) * SUBS + k
            self.arrive(at)
            self.pass_on(at, partner)

        def paired(self, chip_at):
            for k in range(SUBS):
                self.arrive((2 * chip_at + 1 - c) * SUBS + k)

        def drain(self):
            hold(self.ref.at[pl.ds(0, 7 * SUBS)], self.send)

        def block(self, tp):
            rows = self.ref[pl.ds(tp * SUBS, SUBS)]
            return rows.reshape(ROWS, D)

    r1 = Rows(n1, n_recv, n_send.at[0])
    r2 = Rows(n2, n_recv, n_send.at[1])

    loads[3].wait()
    loads[7].wait()

    def norm_in(k):
        for h in range(SUB // 16):
            rows = tok[pl.ds(pl.multiple_of(k * SUB + 16 * h, 16), 16), :].astype(F32)
            n1[t * SUBS + k, pl.ds(16 * h, 16), :] = normed(rows, pre_mix[...]).astype(BF16)
        r1.own(k)

    loop(SUBS, norm_in)

    for i in range(8, 12):
        loads[i].wait()
    for d in range(2):
        gates[:, pl.ds(256 * d, 128)] = w_rec[d, 0]
        gates[:, pl.ds(256 * d + 128, 128)] = w_inp[d, 0]
    low = -decay[...]
    scale[...] = -8.0 * (jnp.maximum(low, 0.0) + jnp.log1p(jnp.exp(-jnp.abs(low))))
    branch[pl.ds(0, 8), :] = jnp.zeros((8, 128), F32)
    branch[pl.ds(1032, 8), :] = jnp.zeros((8, 128), F32)

    ga.first(0)
    ga.first(1)
    own_out.wait()
    for e in range(1, 8):
        other = rem(t + e, 8)
        lanes = pl.ds(pl.multiple_of(other * 128, 128), 128)
        hold(o_all.at[f, c, :, lanes], pre_recv.at[other])
    go.spread_near()
    r1.behind(0)
    r1.ahead(0)
    ga.hop(1, 0)
    ga.hop(1, 1)
    r1.behind(1)
    r1.ahead(1)
    ga.hop(2, 0)
    go.near()
    r1.behind(2)
    r1.ahead(2)
    ga.hop(2, 1)
    r1.behind(3)
    r1.ahead(3)
    for i in (4, 5, 6, 12, 13, 14):
        loads[i].wait()
    ga.hop(3, 0)
    go.late()
    gf.spread_near()
    go.hop(1, 0)
    for k in range(2):
        r1.far(k)
    ga.finish()
    for k in range(2, SUBS):
        r1.far(k)

    def project(chip_at):
        r1.paired(chip_at)
        rows = n1[pl.ds(2 * chip_at * SUBS, 2 * SUBS)].reshape(2 * ROWS, D)
        both = jnp.dot(rows, a_all[...].reshape(D, 256), preferred_element_type=F32)
        both = both.astype(BF16).astype(F32)
        at = chip_at * 2 * ROWS
        branch[pl.ds(pl.multiple_of(at + 8, 8), 2 * ROWS), :] = both[:, :128]
        gel[pl.ds(pl.multiple_of(at, 8), 2 * ROWS), :] = both[:, 128:]

    project(x)
    project(chip(turn))
    go.hop(1, 1)
    project(chip(-turn))
    go.hop(2, 0)
    project(chip(2))

    taps = conv_weight[...].astype(F32)

    def gate(s):
        window = branch[pl.ds(pl.multiple_of(s * 128, 8), 144), :]
        summed = taps[0:1] * window[6:134]
        for offset in range(1, 4):
            summed = summed + taps[offset : offset + 1] * window[6 + offset : 134 + offset]
        conv = summed.astype(BF16)
        wide = conv.astype(F32)
        both = jnp.dot(conv, gates[...], preferred_element_type=F32)
        at = pl.ds(pl.multiple_of(s * SEG, 8), 128)
        for d, (ret, fee) in enumerate(((ret0, fee0), (ret1, fee1))):
            rate = sigmoid(both[:, 256 * d : 256 * d + 128])
            inflow = sigmoid(both[:, 256 * d + 128 : 256 * d + 256])
            log_retain = rate * scale[pl.ds(d, 1), :]
            retain = jnp.exp(log_retain)
            u = 2.0 * log_retain
            near = 1.0 + u * (0.2 * (1.0 + u * (1.0 / 6.0)))
            near = 1.0 + u * (1.0 / 3.0) * (1.0 + u * 0.25 * near)
            near = -u * (1.0 + 0.5 * u * near)
            lost = jnp.where(u > -0.25, near, 1.0 - retain * retain)
            ret[at, :] = retain
            fee[at, :] = jnp.sqrt(lost) * inflow * wide

    loop(4, gate)
    go.hop(2, 1)
    loop(4, lambda s: gate(s + 4))
    gf.near()

    one, zero = jnp.ones((8, 128), F32), jnp.zeros((8, 128), F32)

    def scan(i, carry):
        h0, a0, h1, a1 = carry
        for k in range(8):
            up = pl.ds(i * 8 + k, 8, stride=SEG)
            down = pl.ds(127 - (i * 8 + k), 8, stride=SEG)
            r, v = ret0[up, :], fee0[up, :]
            h0 = r * h0 + v
            a0 = r * a0
            fee0[up, :] = h0
            ret0[up, :] = a0
            r, v = ret1[down, :], fee1[down, :]
            h1 = r * h1 + v
            a1 = r * a1
            fee1[down, :] = h1
            ret1[down, :] = a1
        return h0, a0, h1, a1

    h0, a0, h1, a1 = lax.fori_loop(0, 16, scan, (zero, one, zero, one))
    state = jnp.zeros((1, 128), F32)
    for s in range(8):
        carry_in[s : s + 1, :] = state
        state = a0[s : s + 1] * state + h0[s : s + 1]
    state = jnp.zeros((1, 128), F32)
    for s in reversed(range(8)):
        carry_in[8 + s : 9 + s, :] = state
        state = a1[s : s + 1] * state + h1[s : s + 1]

    def mix(e):
        s = rem(t + e, 8)
        at = pl.ds(pl.multiple_of(s * SEG, 8), 128)
        state = fee0[at, :] + ret0[at, :] * carry_in[pl.ds(s, 1), :]
        state = state + (fee1[at, :] + ret1[at, :] * carry_in[pl.ds(8 + s, 1), :])
        value = gelu(gel[pl.ds(pl.multiple_of(s * 128, 8), 128), :]) * state
        mixed[s] = value.astype(BF16)

        @pl.when(e > 0)
        def _():
            remote(mixed.at[s], hidden.at[t], mix_send, mix_recv.at[t], tp=s).start()

        @pl.when(e == 0)
        def _():
            hidden[s] = value.astype(BF16)

    loop(8, mix)
    go.hop(3, 0)
    gf.late()
    go.finish()

    def swap(part):
        rows = o_all.at[pl.ds(16 * part, 16), c]
        remote(rows, rows, swap_send, swap_recv.at[part], tp=partner).start()

    loop(4, swap)
    gf.hop(1, 0)
    for e in range(1, 8):
        other = rem(t + e, 8)
        hold(hidden.at[other], mix_recv.at[other])

    wide_hidden = jnp.concatenate([hidden[i] for i in range(8)], axis=1)

    def project_out(part):
        hold(o_all.at[pl.ds(16 * part, 16), 1 - c], swap_recv.at[part])
        weight = o_all[pl.ds(16 * part, 16)].reshape(512, 1024)
        msum[:, pl.ds(pl.multiple_of(part * 512, 128), 512)] = lax.dot_general(
            wide_hidden, weight, NT, preferred_element_type=F32
        )

    loop(4, project_out)

    def norm_mid(k):
        for h in range(SUB // 16):
            at = pl.ds(pl.multiple_of(k * SUB + 16 * h, 16), 16)
            total = tok[at, :].astype(F32) + normed(msum[at, :], post_mix[...])
            total = total.astype(BF16)
            res[at, :] = total
            n2[t * SUBS + k, pl.ds(16 * h, 16), :] = normed(
                total.astype(F32), pre_ffn[...]
            ).astype(BF16)
        r2.own(k)

    loop(SUBS, norm_mid)
    gf.hop(1, 1)
    gf.hop(2, 0)
    r2.behind(0)
    r2.ahead(0)
    gf.hop(2, 1)
    r2.behind(1)
    r2.ahead(1)
    r2.behind(2)
    r2.ahead(2)
    gf.hop(3, 0)
    r2.behind(3)
    r2.ahead(3)
    gf.finish()

    def feed_up(i):
        away = 2 if i == 0 else 0 if i == 3 else -turn if i == 1 else turn
        mine = chip(away)
        theirs = chip(-away)
        r2.paired(theirs)
        rows = jnp.concatenate([r2.block(2 * theirs + 1 - c), r2.block(2 * mine + c)], axis=0)
        for n in range(3):
            gu[:, pl.ds(256 * n, 256)] = jnp.dot(
                rows, f_all[:, :, pl.ds(256 * n, 256)].reshape(D, 256), preferred_element_type=F32
            )
        for h in range(4):
            at = pl.ds(64 * h, 64)
            g = gu[at, pl.ds(0, 384)]
            hid[at, :] = (g * sigmoid(g) * gu[at, pl.ds(384, 384)]).astype(BF16)

    def feed_down(i):
        def down(n):
            weight = f_all[pl.ds(16 * n, 16), :, pl.ds(768, 384)].reshape(512, 384)
            part = lax.dot_general(hid[...], weight, NT, preferred_element_type=F32)
            lanes = pl.ds(pl.multiple_of(512 * n, 128), 512)
            give[i, :, lanes] = part[:ROWS].astype(BF16)
            keep[i, :, lanes] = part[ROWS:]

        loop(4, down)
        remote(give.at[i], got.at[i], pair_send, pair_recv.at[i], tp=partner).start()

    def pass_sum(o):
        target = 2 * chip(-turn if o == 1 else turn) + c
        hold(got.at[o], pair_recv.at[o])

        def add(k):
            if o == 2:
                hold(land.at[0, k], land_recv.at[0, k])
            for h in range(SUB // 16):
                at = pl.ds(pl.multiple_of(k * SUB + 16 * h, 16), 16)
                inner = pl.ds(16 * h, 16)
                total = keep[o, at, :] + got[o, at, :].astype(F32)
                if o == 2:
                    total = total + land[0, k, inner, :].astype(F32)
                sums[o, k, inner, :] = total.astype(BF16)
            remote(
                sums.at[o, k], land.at[o, k], land_send, land_recv.at[o, k], tp=target
            ).start()

        loop(SUBS, add)

    feed_up(1)
    feed_down(1)
    for k in range(SUBS):
        r2.far(k)
    feed_up(2)
    pass_sum(1)
    feed_down(2)
    feed_up(0)
    feed_down(0)
    feed_up(3)
    pass_sum(0)
    feed_down(3)
    pass_sum(2)
    hold(got.at[3], pair_recv.at[3])

    def last(k):
        hold(land.at[1, k], land_recv.at[1, k])
        hold(land.at[2, k], land_recv.at[2, k])
        for h in range(SUB // 16):
            at = pl.ds(pl.multiple_of(k * SUB + 16 * h, 16), 16)
            inner = pl.ds(16 * h, 16)
            total = keep[3, at, :] + got[3, at, :].astype(F32)
            total = total + land[1, k, inner, :].astype(F32)
            total = total + land[2, k, inner, :].astype(F32)
            final = res[at, :].astype(F32) + normed(total, post_ffn[...])
            final_rows[at, :] = final.astype(BF16)
        rows = pl.ds(pl.multiple_of(k * SUB, SUB), SUB)
        pltpu.make_async_copy(final_rows.at[rows], out.at[rows], load_sem.at[k]).start()

    loop(SUBS, last)

    for k in range(SUBS):
        hold(final_rows.at[pl.ds(0, SUB)], load_sem.at[k])
    hold(a_all.at[pl.ds(0, 63)], ring_send.at[0])
    hold(o_all.at[pl.ds(0, 63), 0], ring_send.at[1])
    hold(f_all.at[pl.ds(0, 63)], ring_send.at[2])
    hold(o_all.at[0, 0, :, pl.ds(0, 896)], pre_send)
    hold(o_all.at[:, c], swap_send)
    r1.drain()
    r2.drain()
    hold(mixed.at[pl.ds(0, 7)], mix_send)
    hold(give, pair_send)
    hold(sums, land_send)


def per_device(
    tokens,
    pre_mix_gain,
    post_mix_gain,
    pre_ffn_gain,
    post_ffn_gain,
    w_branch,
    w_gelu,
    conv_weight,
    w_rec,
    w_inp,
    decay,
    out_weight_t,
    w_gate,
    w_up,
    down_weight_t,
):
    gains = [
        g.reshape(1, D) for g in (pre_mix_gain, post_mix_gain, pre_ffn_gain, post_ffn_gain)
    ]
    far = pl.BlockSpec(memory_space=pltpu.HBM)
    dma = pltpu.SemaphoreType.DMA
    return pl.pallas_call(
        layer,
        out_shape=jax.ShapeDtypeStruct((ROWS, D), BF16),
        in_specs=[far] * 15,
        out_specs=far,
        scratch_shapes=[
            pltpu.VMEM((1, D), F32),
            pltpu.VMEM((1, D), F32),
            pltpu.VMEM((1, D), F32),
            pltpu.VMEM((1, D), F32),
            pltpu.VMEM((4, 128), BF16),
            pltpu.VMEM((2, 1, 128, 128), BF16),
            pltpu.VMEM((2, 1, 128, 128), BF16),
            pltpu.VMEM((2, 128), F32),
            pltpu.VMEM((ROWS, D), BF16),
            pltpu.VMEM((8 * SUBS, SUB, D), BF16),
            pltpu.VMEM((8 * SUBS, SUB, D), BF16),
            pltpu.VMEM((64, 32, 256), BF16),
            pltpu.VMEM((64, 2, 16, 1024), BF16),
            pltpu.VMEM((64, 32, 1152), BF16),
            pltpu.VMEM((2, 16, 128), BF16),
            pltpu.VMEM((1040, 128), F32),
            pltpu.VMEM((1024, 128), F32),
            pltpu.VMEM((8 * SEG, 128), F32),
            pltpu.VMEM((8 * SEG, 128), F32),
            pltpu.VMEM((8 * SEG, 128), F32),
            pltpu.VMEM((8 * SEG, 128), F32),
            pltpu.VMEM((128, 512), BF16),
            pltpu.VMEM((2, 128), F32),
            pltpu.VMEM((16, 128), F32),
            pltpu.VMEM((8, 128, 128), BF16),
            pltpu.VMEM((8, 128, 128), BF16),
            pltpu.VMEM((ROWS, D), F32),
            pltpu.VMEM((ROWS, D), BF16),
            pltpu.VMEM((2 * ROWS, 768), F32),
            pltpu.VMEM((2 * ROWS, 384), BF16),
            pltpu.VMEM((4, ROWS, D), F32),
            pltpu.VMEM((4, ROWS, D), BF16),
            pltpu.VMEM((4, ROWS, D), BF16),
            pltpu.VMEM((3, SUBS, SUB, D), BF16),
            pltpu.VMEM((3, SUBS, SUB, D), BF16),
            pltpu.VMEM((ROWS, D), BF16),
            dma((16,)),
            dma((64,)),
            dma((64,)),
            dma((64,)),
            dma((3,)),
            dma((8,)),
            dma,
            dma((4,)),
            dma,
            dma((8 * SUBS,)),
            dma((2,)),
            dma((8,)),
            dma,
            dma((4,)),
            dma,
            dma((3, SUBS)),
            dma,
        ],
        compiler_params=pltpu.CompilerParams(
            collective_id=0, has_side_effects=True, vmem_limit_bytes=60 * 1024 * 1024
        ),
    )(
        tokens,
        *gains,
        w_branch,
        w_gelu,
        conv_weight,
        w_rec,
        w_inp,
        decay,
        out_weight_t.reshape(2, 16, 128),
        w_gate,
        w_up,
        down_weight_t,
    )


def solution(mesh):
    return jax.shard_map(
        per_device,
        mesh=mesh,
        in_specs=(
            P(("fs", "tp"), None),
            P(),
            P(),
            P(),
            P(),
            P("fs", "tp"),
            P("fs", "tp"),
            P(None, "tp"),
            P(None, "tp", None, None),
            P(None, "tp", None, None),
            P(None, "tp"),
            P("fs", "tp"),
            P("fs", "tp"),
            P("fs", "tp"),
            P("fs", "tp"),
        ),
        out_specs=P(("fs", "tp"), None),
        check_vma=False,
    )
```

```python
import jax
import jax.numpy as jnp
from jax import lax
from jax.experimental import pallas as pl
from jax.experimental.pallas import tpu as pltpu
from jax.sharding import PartitionSpec as P

EPS = 1e-06
MESH = pl.DeviceIdType.MESH
F32 = jnp.float32
BF16 = jnp.bfloat16
RING = 8
CHIPS = 4
ROWS = 128
SUB = 32
SUBS = ROWS // SUB
D = 2048
SEG = 136
WIDE = (2, -2, 1, -1)
NT = (((1,), (1,)), ((), ()))


def rem(a, n):
    return lax.rem(a, jnp.int32(n))


def hold(ref, sem):
    pltpu.make_async_copy(ref, ref, sem).wait()


def normed(values, gain):
    factor = lax.rsqrt(jnp.mean(values * values, axis=-1, keepdims=True) + EPS)
    return values * factor * gain


def sigmoid(v):
    return 0.5 + 0.5 * jnp.tanh(0.5 * v)


def gelu(v):
    return 0.5 * v * (1.0 + jnp.tanh(0.7978845608028654 * (v + 0.044715 * v * v * v)))


def loop(count, body):
    def step(i, carry):
        body(i)
        return carry

    lax.fori_loop(0, count, step, 0)


def layer(
    tokens,
    pre_mix_hbm,
    post_mix_hbm,
    pre_ffn_hbm,
    post_ffn_hbm,
    w_branch,
    w_gelu,
    conv_hbm,
    w_rec_hbm,
    w_inp_hbm,
    decay_hbm,
    out_w,
    w_gate,
    w_up,
    w_down,
    out,
    pre_mix,
    post_mix,
    pre_ffn,
    post_ffn,
    conv_weight,
    w_rec,
    w_inp,
    decay,
    tok,
    n1,
    n2,
    a_all,
    o_all,
    f_all,
    o_own,
    branch,
    gel,
    ret0,
    ret1,
    fee0,
    fee1,
    gates,
    scale,
    carry_in,
    mixed,
    hidden,
    msum,
    res,
    gu,
    hid,
    keep,
    give,
    got,
    sums,
    land,
    power,
    final_rows,
    load_sem,
    a_recv,
    o_recv,
    f_recv,
    ring_send,
    pre_recv,
    pre_send,
    swap_recv,
    swap_send,
    n_recv,
    n_send,
    mix_recv,
    mix_send,
    pair_recv,
    pair_send,
    land_recv,
    land_send,
):
    f = lax.axis_index("fs")
    t = lax.axis_index("tp")
    z, y = lax.div(f, jnp.int32(RING)), rem(f, RING)
    x, c = lax.div(t, jnp.int32(2)), rem(t, 2)
    p, q = y + c * (z - y), z + c * (y - z)
    step_p, step_q = 1 + (RING - 1) * c, RING - (RING - 1) * c
    turn = 1 - 2 * c
    partner = 2 * x + 1 - c

    def place(pp, qq):
        return pp * step_p + qq * step_q

    def remote(src, dst, send, recv, fs=None, tp=None):
        return pltpu.make_async_remote_copy(
            src_ref=src,
            dst_ref=dst,
            send_sem=send,
            recv_sem=recv,
            device_id={"fs": f if fs is None else fs, "tp": t if tp is None else tp},
            device_id_type=MESH,
        )

    def chip(away):
        return rem(x + away + CHIPS, CHIPS)

    loads = [
        (w_branch, a_all.at[f, :, pl.ds(0, 128)]),
        (w_gelu, a_all.at[f, :, pl.ds(128, 128)]),
        (out_w, o_own),
        (tokens, tok),
        (w_gate, f_all.at[f, :, pl.ds(0, 384)]),
        (w_up, f_all.at[f, :, pl.ds(384, 384)]),
        (w_down, f_all.at[f, :, pl.ds(768, 384)]),
        (pre_mix_hbm, pre_mix),
        (conv_hbm, conv_weight),
        (w_rec_hbm, w_rec),
        (w_inp_hbm, w_inp),
        (decay_hbm, decay),
        (post_mix_hbm, post_mix),
        (pre_ffn_hbm, pre_ffn),
        (post_ffn_hbm, post_ffn),
    ]
    loads = [pltpu.make_async_copy(s, d, load_sem.at[i]) for i, (s, d) in enumerate(loads)]
    for copy in loads:
        copy.start()

    barrier = pltpu.get_barrier_semaphore()

    def greet(fs, tp):
        pl.semaphore_signal(barrier, inc=1, device_id={"fs": fs, "tp": tp}, device_id_type=MESH)

    for e in range(1, RING):
        greet(place(rem(p + e, RING), q), t)
    for e in (1, 2, RING - 2, RING - 1):
        greet(place(p, rem(q + e, RING)), t)
    for e in range(1, 8):
        greet(f, rem(t + e, 8))
    loads[3].wait()
    loads[7].wait()

    def norm_in(k):
        for h in range(SUB // 16):
            rows = tok[pl.ds(pl.multiple_of(k * SUB + 16 * h, 16), 16), :].astype(F32)
            n1[t * SUBS + k, pl.ds(16 * h, 16), :] = normed(rows, pre_mix[...]).astype(BF16)

    loop(SUBS, norm_in)

    for i in range(8, 12):
        loads[i].wait()
    for d in range(2):
        gates[:, pl.ds(256 * d, 128)] = w_rec[d, 0]
        gates[:, pl.ds(256 * d + 128, 128)] = w_inp[d, 0]
    low = -decay[...]
    scale[...] = -8.0 * (jnp.maximum(low, 0.0) + jnp.log1p(jnp.exp(-jnp.abs(low))))
    branch[pl.ds(0, 8), :] = jnp.zeros((8, 128), F32)
    branch[pl.ds(1032, 8), :] = jnp.zeros((8, 128), F32)

    pl.semaphore_wait(barrier, 18)

    class Gather:
        def __init__(self, piece, recv, send, share=None):
            self.piece, self.recv, self.send = piece, recv, send
            self.share = share or (lambda slot: None)

        def spread(self):
            def body(e):
                j = e + 1
                off = lax.div(j + 1, jnp.int32(2)) * (2 * rem(j, 2) - 1)
                there = place(rem(p + off + RING, RING), q)
                remote(self.piece(f), self.piece(f), self.send, self.recv.at[f], fs=there).start()

            loop(RING - 1, body)

        def slot(self, j, away):
            off = lax.div(j + 1, jnp.int32(2)) * (2 * rem(j, 2) - 1)
            return place(rem(p + off + RING, RING), rem(q + away + RING, RING))

        def pass_on(self, slot, way):
            there = place(p, rem(q + way + RING, RING))
            remote(
                self.piece(slot), self.piece(slot), self.send, self.recv.at[slot], fs=there
            ).start()

        def arrive(self, slot):
            hold(self.piece(slot), self.recv.at[slot])
            self.share(slot)

        def first(self, half):
            def body(i):
                j = i + 4 * half
                slot = self.slot(j, 0)

                @pl.when(j > 0)
                def _():
                    self.arrive(slot)

                self.pass_on(slot, 1)
                self.pass_on(slot, -1)

            loop(4, body)

        def first_wide(self, half):
            def body(i):
                j = i + 4 * half
                slot = self.slot(j, 0)

                @pl.when(j > 0)
                def _():
                    self.arrive(slot)

                for way in (2, -2, 1, -1):
                    self.pass_on(slot, way)

            loop(4, body)

        def relay_wide(self, low, count):
            def body(i):
                j = i + low
                for way in (1, -1):
                    slot = self.slot(j, -2 * way)
                    self.arrive(slot)
                    self.pass_on(slot, way)

                    @pl.when(rem(j, 2) == (0 if way > 0 else 1))
                    def _():
                        self.pass_on(slot, 2 * way)

            loop(count, body)

        def finish_wide(self):
            def body(j):
                for away in (1, -1, 3, -3, 4):
                    self.arrive(self.slot(j, away))

            loop(8, body)

        def spread_near(self):
            for e in (1, -1, 2, -2):
                there = place(rem(p + e + RING, RING), q)
                remote(self.piece(f), self.piece(f), self.send, self.recv.at[f], fs=there).start()

        def relay(self, slot, e):
            there = place(rem(p + e + RING, RING), q)
            remote(
                self.piece(slot), self.piece(slot), self.send, self.recv.at[slot], fs=there
            ).start()

        def near(self, ways=(1, -1)):
            for j, off in enumerate((0, 1, -1, 2, -2)):
                slot = place(rem(p + off + RING, RING), q)
                if j > 0:
                    self.arrive(slot)
                else:
                    self.share(slot)
                if j > 2:
                    way = 1 if off < 0 else -1
                    self.relay(slot, way)

                    @pl.when(rem(p, 2) == (0 if off < 0 else 1))
                    def _():
                        self.relay(slot, 2 * way)

                for way in ways:
                    self.pass_on(slot, way)

        def late(self, ways=(1, -1)):
            for off in (3, -3, 4):
                slot = place(rem(p + off + RING, RING), q)
                self.arrive(slot)
                for way in ways:
                    self.pass_on(slot, way)

        def hop(self, far, half):
            def body(i):
                j = i + 4 * half
                k = j + 4 if far == 3 else j
                from_left, from_right = self.slot(j, -far), self.slot(k, far)
                self.arrive(from_left)
                self.pass_on(from_left, 1)
                self.arrive(from_right)
                self.pass_on(from_right, -1)

            loop(4, body)

        def finish(self):
            def body(j):
                self.arrive(self.slot(j + 4, -3))
                self.arrive(self.slot(j, 3))
                self.arrive(self.slot(j, 4))
                self.arrive(self.slot(j + 4, 4))

            loop(4, body)

    ga = Gather(lambda s: a_all.at[s], a_recv, ring_send.at[0])
    def share(slot):
        rows = o_all.at[slot, c]
        remote(rows, rows, swap_send, swap_recv, tp=partner).start()

    go = Gather(lambda s: o_all.at[s, c], o_recv, ring_send.at[1], share)
    gf = Gather(lambda s: f_all.at[s], f_recv, ring_send.at[2])

    loads[0].wait()
    loads[1].wait()
    ga.spread()

    loads[2].wait()
    own_lanes = pl.ds(pl.multiple_of(t * 128, 128), 128)
    for e in range(1, 8):
        other = rem(t + e, 8)
        half = rem(other, 2)
        remote(
            o_own.at[half], o_all.at[f, half, :, own_lanes], pre_send, pre_recv.at[t], tp=other
        ).start()
    own_out = pltpu.make_async_copy(o_own.at[c], o_all.at[f, c, :, own_lanes], load_sem.at[15])
    own_out.start()

    class Rows:
        def __init__(self, ref, recv, send):
            self.ref, self.recv, self.send = ref, recv, send

        def pass_on(self, at, tp):
            remote(self.ref.at[at], self.ref.at[at], self.send, self.recv.at[at], tp=tp).start()

        def arrive(self, at):
            hold(self.ref.at[at], self.recv.at[at])

        def own(self, k):
            at = t * SUBS + k
            self.pass_on(at, 2 * chip(turn) + c)
            self.pass_on(at, 2 * chip(-turn) + c)
            self.pass_on(at, partner)

        def behind(self, k):
            at = (2 * chip(-turn) + c) * SUBS + k
            self.arrive(at)
            self.pass_on(at, 2 * chip(turn) + c)
            self.pass_on(at, partner)

        def ahead(self, k):
            at = (2 * chip(turn) + c) * SUBS + k
            self.arrive(at)
            self.pass_on(at, partner)

        def far(self, k):
            at = (2 * chip(2) + c) * SUBS + k
            self.arrive(at)
            self.pass_on(at, partner)

        def paired(self, chip_at):
            for k in range(SUBS):
                self.arrive((2 * chip_at + 1 - c) * SUBS + k)

        def drain(self):
            hold(self.ref.at[pl.ds(0, 7 * SUBS)], self.send)

        def block(self, tp):
            rows = self.ref[pl.ds(tp * SUBS, SUBS)]
            return rows.reshape(ROWS, D)

    r1 = Rows(n1, n_recv, n_send.at[0])
    r2 = Rows(n2, n_recv, n_send.at[1])

    loop(SUBS, r1.own)

    for i in (4, 5, 6, 12, 13, 14):
        loads[i].wait()
    gf.spread_near()
    ga.first_wide(0)
    ga.first_wide(1)
    own_out.wait()
    for e in range(1, 8):
        other = rem(t + e, 8)
        lanes = pl.ds(pl.multiple_of(other * 128, 128), 128)
        hold(o_all.at[f, c, :, lanes], pre_recv.at[other])
    go.spread_near()
    r1.behind(0)
    r1.ahead(0)
    ga.relay_wide(0, 4)
    ga.relay_wide(4, 4)
    r1.behind(1)
    r1.ahead(1)
    go.near()
    gf.near()
    r1.behind(2)
    r1.ahead(2)
    r1.behind(3)
    r1.ahead(3)
    ga.finish_wide()
    go.late()
    go.hop(1, 0)

    def project(chip_at):
        r1.paired(chip_at)
        rows = n1[pl.ds(2 * chip_at * SUBS, 2 * SUBS)].reshape(2 * ROWS, D)
        both = jnp.dot(rows, a_all[...].reshape(D, 256), preferred_element_type=F32)
        both = both.astype(BF16).astype(F32)
        at = chip_at * 2 * ROWS
        branch[pl.ds(pl.multiple_of(at + 8, 8), 2 * ROWS), :] = both[:, :128]
        gel[pl.ds(pl.multiple_of(at, 8), 2 * ROWS), :] = both[:, 128:]

    r1.far(0)
    r1.far(1)
    project(x)
    r1.far(2)
    project(chip(turn))
    r1.far(3)
    project(chip(-turn))
    go.hop(1, 1)
    project(chip(2))
    go.hop(2, 0)

    taps = conv_weight[...].astype(F32)

    def gate(s):
        window = branch[pl.ds(pl.multiple_of(s * 128, 8), 144), :]
        summed = taps[0:1] * window[6:134]
        for offset in range(1, 4):
            summed = summed + taps[offset : offset + 1] * window[6 + offset : 134 + offset]
        conv = summed.astype(BF16)
        wide = conv.astype(F32)
        both = jnp.dot(conv, gates[...], preferred_element_type=F32)
        at = pl.ds(pl.multiple_of(s * SEG, 8), 128)
        for d, (ret, fee) in enumerate(((ret0, fee0), (ret1, fee1))):
            rate = sigmoid(both[:, 256 * d : 256 * d + 128])
            inflow = sigmoid(both[:, 256 * d + 128 : 256 * d + 256])
            log_retain = rate * scale[pl.ds(d, 1), :]
            retain = jnp.exp(log_retain)
            u = 2.0 * log_retain
            near = 1.0 + u * (0.2 * (1.0 + u * (1.0 / 6.0)))
            near = 1.0 + u * (1.0 / 3.0) * (1.0 + u * 0.25 * near)
            near = -u * (1.0 + 0.5 * u * near)
            lost = jnp.where(u > -0.25, near, 1.0 - retain * retain)
            ret[at, :] = retain
            fee[at, :] = jnp.sqrt(lost) * inflow * wide

    loop(4, gate)
    go.hop(2, 1)
    loop(4, lambda s: gate(s + 4))

    one, zero = jnp.ones((8, 128), F32), jnp.zeros((8, 128), F32)

    def scan(i, carry):
        h0, a0, h1, a1 = carry
        for k in range(8):
            up = pl.ds(i * 8 + k, 8, stride=SEG)
            down = pl.ds(127 - (i * 8 + k), 8, stride=SEG)
            r, v = ret0[up, :], fee0[up, :]
            h0 = r * h0 + v
            a0 = r * a0
            fee0[up, :] = h0
            ret0[up, :] = a0
            r, v = ret1[down, :], fee1[down, :]
            h1 = r * h1 + v
            a1 = r * a1
            fee1[down, :] = h1
            ret1[down, :] = a1
        return h0, a0, h1, a1

    h0, a0, h1, a1 = lax.fori_loop(0, 16, scan, (zero, one, zero, one))
    state = jnp.zeros((1, 128), F32)
    for s in range(8):
        carry_in[s : s + 1, :] = state
        state = a0[s : s + 1] * state + h0[s : s + 1]
    state = jnp.zeros((1, 128), F32)
    for s in reversed(range(8)):
        carry_in[8 + s : 9 + s, :] = state
        state = a1[s : s + 1] * state + h1[s : s + 1]

    def mix(e):
        m = lax.div(e, jnp.int32(2))
        away = jnp.where(m == 3, 0, jnp.where(m == 2, 3, 2 - m))
        s = 2 * chip(away) + rem(c + 1 + e, 2)
        at = pl.ds(pl.multiple_of(s * SEG, 8), 128)
        state = fee0[at, :] + ret0[at, :] * carry_in[pl.ds(s, 1), :]
        state = state + (fee1[at, :] + ret1[at, :] * carry_in[pl.ds(8 + s, 1), :])
        value = gelu(gel[pl.ds(pl.multiple_of(s * 128, 8), 128), :]) * state
        mixed[s] = value.astype(BF16)

        @pl.when(e < 7)
        def _():
            remote(mixed.at[s], hidden.at[t], mix_send, mix_recv.at[t], tp=s).start()

        @pl.when(e == 7)
        def _():
            hidden[s] = value.astype(BF16)

    loop(8, mix)
    go.hop(3, 0)
    gf.late()
    go.finish()
    gf.hop(1, 0)
    for e in range(1, 8):
        other = rem(t + e, 8)
        hold(hidden.at[other], mix_recv.at[other])

    wide_hidden = jnp.concatenate([hidden[i] for i in range(8)], axis=1)

    hold(o_all.at[:, 1 - c], swap_recv)

    def project_out(part):
        weight = o_all[pl.ds(16 * part, 16)].reshape(512, 1024)
        msum[:, pl.ds(pl.multiple_of(part * 512, 128), 512)] = lax.dot_general(
            wide_hidden, weight, NT, preferred_element_type=F32
        )

    loop(4, project_out)

    def norm_mid(k):
        for h in range(SUB // 16):
            at = pl.ds(pl.multiple_of(k * SUB + 16 * h, 16), 16)
            total = tok[at, :].astype(F32) + normed(msum[at, :], post_mix[...])
            total = total.astype(BF16)
            res[at, :] = total
            n2[t * SUBS + k, pl.ds(16 * h, 16), :] = normed(
                total.astype(F32), pre_ffn[...]
            ).astype(BF16)
        r2.own(k)

    loop(SUBS, norm_mid)
    gf.hop(1, 1)
    gf.hop(2, 0)
    r2.behind(0)
    r2.ahead(0)
    gf.hop(2, 1)
    r2.behind(1)
    r2.ahead(1)
    r2.behind(2)
    r2.ahead(2)
    gf.hop(3, 0)
    r2.behind(3)
    r2.ahead(3)
    gf.finish()

    def feed_up(i):
        away = 2 if i == 0 else 0 if i == 3 else -turn if i == 1 else turn
        mine = chip(away)
        theirs = chip(-away)
        r2.paired(theirs)
        rows = jnp.concatenate([r2.block(2 * theirs + 1 - c), r2.block(2 * mine + c)], axis=0)
        for n in range(3):
            gu[:, pl.ds(256 * n, 256)] = jnp.dot(
                rows, f_all[:, :, pl.ds(256 * n, 256)].reshape(D, 256), preferred_element_type=F32
            )
        for h in range(4):
            at = pl.ds(64 * h, 64)
            g = gu[at, pl.ds(0, 384)]
            hid[at, :] = (g * sigmoid(g) * gu[at, pl.ds(384, 384)]).astype(BF16)

    def feed_down(i):
        def down(n):
            weight = f_all[pl.ds(16 * n, 16), :, pl.ds(768, 384)].reshape(512, 384)
            part = lax.dot_general(hid[...], weight, NT, preferred_element_type=F32)
            give[i, n] = part[:ROWS].astype(BF16)
            keep[i, n] = part[ROWS:]
            remote(
                give.at[i, n], got.at[i, n], pair_send, pair_recv.at[i, n], tp=partner
            ).start()

        loop(4, down)

    def pass_sum(o, low, count):
        target = 2 * chip(-turn if o == 1 else turn) + c

        def add(m):
            n = m + low
            hold(got.at[o, n], pair_recv.at[o, n])
            if o == 2:
                hold(land.at[0, n], land_recv.at[0, n])
            for h in range(ROWS // SUB):
                at = pl.ds(SUB * h, SUB)
                total = keep[o, n, at, :] + got[o, n, at, :].astype(F32)
                if o == 2:
                    total = total + land[0, n, at, :].astype(F32)
                sums[o, n, at, :] = total.astype(BF16)
            remote(
                sums.at[o, n], land.at[o, n], land_send, land_recv.at[o, n], tp=target
            ).start()

        loop(count, add)

    feed_up(1)
    feed_down(1)
    for k in range(SUBS):
        r2.far(k)
    pass_sum(1, 0, 2)
    feed_up(2)
    pass_sum(1, 2, 2)
    feed_down(2)
    feed_up(0)
    feed_down(0)
    pass_sum(0, 0, 2)
    feed_up(3)
    pass_sum(0, 2, 2)
    feed_down(3)
    pass_sum(2, 0, 4)

    power[...] = jnp.zeros_like(power)

    def own_sum(n):
        hold(got.at[3, n], pair_recv.at[3, n])
        hold(land.at[1, n], land_recv.at[1, n])
        hold(land.at[2, n], land_recv.at[2, n])
        for h in range(ROWS // SUB):
            at = pl.ds(SUB * h, SUB)
            total = keep[3, n, at, :] + got[3, n, at, :].astype(F32)
            total = total + land[1, n, at, :].astype(F32)
            total = total + land[2, n, at, :].astype(F32)
            keep[3, n, at, :] = total
            square = total * total
            square = square[:, :256] + square[:, 256:]
            power[at, :] += square[:, :128] + square[:, 128:]

    loop(4, own_sum)

    def last(k):
        for h in range(SUB // 16):
            at = pl.ds(pl.multiple_of(k * SUB + 16 * h, 16), 16)
            mean = jnp.sum(power[at, :], axis=-1, keepdims=True) * (1.0 / D)
            factor = lax.rsqrt(mean + EPS)
            for n in range(4):
                lanes = pl.ds(512 * n, 512)
                value = keep[3, n, at, :] * factor * post_ffn[:, lanes]
                final_rows[at, lanes] = (res[at, lanes].astype(F32) + value).astype(BF16)
        rows = pl.ds(pl.multiple_of(k * SUB, SUB), SUB)
        pltpu.make_async_copy(final_rows.at[rows], out.at[rows], load_sem.at[k]).start()

    loop(SUBS, last)

    for k in range(SUBS):
        hold(final_rows.at[pl.ds(0, SUB)], load_sem.at[k])
    hold(a_all.at[pl.ds(0, 63)], ring_send.at[0])
    hold(o_all.at[pl.ds(0, 63), 0], ring_send.at[1])
    hold(f_all.at[pl.ds(0, 63)], ring_send.at[2])
    hold(o_all.at[0, 0, :, pl.ds(0, 896)], pre_send)
    hold(o_all.at[:, c], swap_send)
    r1.drain()
    r2.drain()
    hold(mixed.at[pl.ds(0, 7)], mix_send)
    hold(give, pair_send)
    hold(sums, land_send)


def per_device(
    tokens,
    pre_mix_gain,
    post_mix_gain,
    pre_ffn_gain,
    post_ffn_gain,
    w_branch,
    w_gelu,
    conv_weight,
    w_rec,
    w_inp,
    decay,
    out_weight_t,
    w_gate,
    w_up,
    down_weight_t,
):
    gains = [
        g.reshape(1, D) for g in (pre_mix_gain, post_mix_gain, pre_ffn_gain, post_ffn_gain)
    ]
    far = pl.BlockSpec(memory_space=pltpu.HBM)
    dma = pltpu.SemaphoreType.DMA
    return pl.pallas_call(
        layer,
        out_shape=jax.ShapeDtypeStruct((ROWS, D), BF16),
        in_specs=[far] * 15,
        out_specs=far,
        scratch_shapes=[
            pltpu.VMEM((1, D), F32),
            pltpu.VMEM((1, D), F32),
            pltpu.VMEM((1, D), F32),
            pltpu.VMEM((1, D), F32),
            pltpu.VMEM((4, 128), BF16),
            pltpu.VMEM((2, 1, 128, 128), BF16),
            pltpu.VMEM((2, 1, 128, 128), BF16),
            pltpu.VMEM((2, 128), F32),
            pltpu.VMEM((ROWS, D), BF16),
            pltpu.VMEM((8 * SUBS, SUB, D), BF16),
            pltpu.VMEM((8 * SUBS, SUB, D), BF16),
            pltpu.VMEM((64, 32, 256), BF16),
            pltpu.VMEM((64, 2, 16, 1024), BF16),
            pltpu.VMEM((64, 32, 1152), BF16),
            pltpu.VMEM((2, 16, 128), BF16),
            pltpu.VMEM((1040, 128), F32),
            pltpu.VMEM((1024, 128), F32),
            pltpu.VMEM((8 * SEG, 128), F32),
            pltpu.VMEM((8 * SEG, 128), F32),
            pltpu.VMEM((8 * SEG, 128), F32),
            pltpu.VMEM((8 * SEG, 128), F32),
            pltpu.VMEM((128, 512), BF16),
            pltpu.VMEM((2, 128), F32),
            pltpu.VMEM((16, 128), F32),
            pltpu.VMEM((8, 128, 128), BF16),
            pltpu.VMEM((8, 128, 128), BF16),
            pltpu.VMEM((ROWS, D), F32),
            pltpu.VMEM((ROWS, D), BF16),
            pltpu.VMEM((2 * ROWS, 768), F32),
            pltpu.VMEM((2 * ROWS, 384), BF16),
            pltpu.VMEM((4, 4, ROWS, 512), F32),
            pltpu.VMEM((4, 4, ROWS, 512), BF16),
            pltpu.VMEM((4, 4, ROWS, 512), BF16),
            pltpu.VMEM((3, 4, ROWS, 512), BF16),
            pltpu.VMEM((3, 4, ROWS, 512), BF16),
            pltpu.VMEM((ROWS, 128), F32),
            pltpu.VMEM((ROWS, D), BF16),
            dma((16,)),
            dma((64,)),
            dma((64,)),
            dma((64,)),
            dma((3,)),
            dma((8,)),
            dma,
            dma,
            dma,
            dma((8 * SUBS,)),
            dma((2,)),
            dma((8,)),
            dma,
            dma((4, 4)),
            dma,
            dma((3, 4)),
            dma,
        ],
        compiler_params=pltpu.CompilerParams(
            collective_id=0, has_side_effects=True, vmem_limit_bytes=60 * 1024 * 1024
        ),
    )(
        tokens,
        *gains,
        w_branch,
        w_gelu,
        conv_weight,
        w_rec,
        w_inp,
        decay,
        out_weight_t.reshape(2, 16, 128),
        w_gate,
        w_up,
        down_weight_t,
    )


def solution(mesh):
    return jax.shard_map(
        per_device,
        mesh=mesh,
        in_specs=(
            P(("fs", "tp"), None),
            P(),
            P(),
            P(),
            P(),
            P("fs", "tp"),
            P("fs", "tp"),
            P(None, "tp"),
            P(None, "tp", None, None),
            P(None, "tp", None, None),
            P(None, "tp"),
            P("fs", "tp"),
            P("fs", "tp"),
            P("fs", "tp"),
            P("fs", "tp"),
        ),
        out_specs=P(("fs", "tp"), None),
        check_vma=False,
    )
```

```python
import jax
import jax.numpy as jnp
from jax import lax
from jax.experimental import pallas as pl
from jax.experimental.pallas import tpu as pltpu
from jax.sharding import PartitionSpec as P

EPS = 1e-06
MESH = pl.DeviceIdType.MESH
F32 = jnp.float32
BF16 = jnp.bfloat16
RING = 8
CHIPS = 4
ROWS = 128
SUB = 32
SUBS = ROWS // SUB
D = 2048
SEG = 136
WIDE = (2, -2, 1, -1)
NT = (((1,), (1,)), ((), ()))


def rem(a, n):
    return lax.rem(a, jnp.int32(n))


def hold(ref, sem):
    pltpu.make_async_copy(ref, ref, sem).wait()


def normed(values, gain):
    factor = lax.rsqrt(jnp.mean(values * values, axis=-1, keepdims=True) + EPS)
    return values * factor * gain


def sigmoid(v):
    return 0.5 + 0.5 * jnp.tanh(0.5 * v)


def gelu(v):
    return 0.5 * v * (1.0 + jnp.tanh(0.7978845608028654 * (v + 0.044715 * v * v * v)))


def loop(count, body):
    def step(i, carry):
        body(i)
        return carry

    lax.fori_loop(0, count, step, 0)


def layer(
    tokens,
    pre_mix_hbm,
    post_mix_hbm,
    pre_ffn_hbm,
    post_ffn_hbm,
    w_branch,
    w_gelu,
    conv_hbm,
    w_rec_hbm,
    w_inp_hbm,
    decay_hbm,
    out_w,
    w_gate,
    w_up,
    w_down,
    out,
    pre_mix,
    post_mix,
    pre_ffn,
    post_ffn,
    conv_weight,
    w_rec,
    w_inp,
    decay,
    tok,
    n1,
    n2,
    a_all,
    o_all,
    f_all,
    o_own,
    branch,
    gel,
    ret0,
    ret1,
    fee0,
    fee1,
    gates,
    scale,
    carry_in,
    mixed,
    hidden,
    msum,
    res,
    gu,
    hid,
    keep,
    give,
    got,
    sums,
    land,
    power,
    final_rows,
    load_sem,
    a_recv,
    o_recv,
    f_recv,
    ring_send,
    pre_recv,
    pre_send,
    swap_recv,
    swap_send,
    n_recv,
    n_send,
    mix_recv,
    mix_send,
    pair_recv,
    pair_send,
    land_recv,
    land_send,
):
    f = lax.axis_index("fs")
    t = lax.axis_index("tp")
    z, y = lax.div(f, jnp.int32(RING)), rem(f, RING)
    x, c = lax.div(t, jnp.int32(2)), rem(t, 2)
    p, q = y + c * (z - y), z + c * (y - z)
    step_p, step_q = 1 + (RING - 1) * c, RING - (RING - 1) * c
    turn = 1 - 2 * c
    partner = 2 * x + 1 - c

    def place(pp, qq):
        return pp * step_p + qq * step_q

    def remote(src, dst, send, recv, fs=None, tp=None):
        return pltpu.make_async_remote_copy(
            src_ref=src,
            dst_ref=dst,
            send_sem=send,
            recv_sem=recv,
            device_id={"fs": f if fs is None else fs, "tp": t if tp is None else tp},
            device_id_type=MESH,
        )

    def chip(away):
        return rem(x + away + CHIPS, CHIPS)

    loads = [
        (w_branch, a_all.at[f, :, pl.ds(0, 128)]),
        (w_gelu, a_all.at[f, :, pl.ds(128, 128)]),
        (out_w, o_own),
        (tokens, tok),
        (w_gate, f_all.at[f, :, pl.ds(0, 384)]),
        (w_up, f_all.at[f, :, pl.ds(384, 384)]),
        (w_down, f_all.at[f, :, pl.ds(768, 384)]),
        (pre_mix_hbm, pre_mix),
        (conv_hbm, conv_weight),
        (w_rec_hbm, w_rec),
        (w_inp_hbm, w_inp),
        (decay_hbm, decay),
        (post_mix_hbm, post_mix),
        (pre_ffn_hbm, pre_ffn),
        (post_ffn_hbm, post_ffn),
    ]
    loads = [pltpu.make_async_copy(s, d, load_sem.at[i]) for i, (s, d) in enumerate(loads)]
    for copy in loads:
        copy.start()

    barrier = pltpu.get_barrier_semaphore()

    def greet(fs, tp):
        pl.semaphore_signal(barrier, inc=1, device_id={"fs": fs, "tp": tp}, device_id_type=MESH)

    for e in range(1, RING):
        greet(place(rem(p + e, RING), q), t)
    for e in (1, 2, RING - 2, RING - 1):
        greet(place(p, rem(q + e, RING)), t)
    for e in range(1, 8):
        greet(f, rem(t + e, 8))
    loads[3].wait()
    loads[7].wait()

    def norm_in(k):
        for h in range(SUB // 16):
            rows = tok[pl.ds(pl.multiple_of(k * SUB + 16 * h, 16), 16), :].astype(F32)
            n1[t * SUBS + k, pl.ds(16 * h, 16), :] = normed(rows, pre_mix[...]).astype(BF16)

    loop(SUBS, norm_in)

    for i in range(8, 12):
        loads[i].wait()
    for d in range(2):
        gates[:, pl.ds(256 * d, 128)] = w_rec[d, 0]
        gates[:, pl.ds(256 * d + 128, 128)] = w_inp[d, 0]
    low = -decay[...]
    scale[...] = -8.0 * (jnp.maximum(low, 0.0) + jnp.log1p(jnp.exp(-jnp.abs(low))))
    branch[pl.ds(0, 8), :] = jnp.zeros((8, 128), F32)
    branch[pl.ds(1032, 8), :] = jnp.zeros((8, 128), F32)

    pl.semaphore_wait(barrier, 18)

    class Gather:
        def __init__(self, piece, recv, send, share=None):
            self.piece, self.recv, self.send = piece, recv, send
            self.share = share or (lambda slot: None)

        def spread(self):
            def body(e):
                j = e + 1
                off = lax.div(j + 1, jnp.int32(2)) * (2 * rem(j, 2) - 1)
                there = place(rem(p + off + RING, RING), q)
                remote(self.piece(f), self.piece(f), self.send, self.recv.at[f], fs=there).start()

            loop(RING - 1, body)

        def slot(self, j, away):
            off = lax.div(j + 1, jnp.int32(2)) * (2 * rem(j, 2) - 1)
            return place(rem(p + off + RING, RING), rem(q + away + RING, RING))

        def pass_on(self, slot, way):
            there = place(p, rem(q + way + RING, RING))
            remote(
                self.piece(slot), self.piece(slot), self.send, self.recv.at[slot], fs=there
            ).start()

        def arrive(self, slot):
            hold(self.piece(slot), self.recv.at[slot])
            self.share(slot)

        def first(self, half):
            def body(i):
                j = i + 4 * half
                slot = self.slot(j, 0)

                @pl.when(j > 0)
                def _():
                    self.arrive(slot)

                self.pass_on(slot, 1)
                self.pass_on(slot, -1)

            loop(4, body)

        def first_wide(self, half):
            def body(i):
                j = i + 4 * half
                slot = self.slot(j, 0)

                @pl.when(j > 0)
                def _():
                    self.arrive(slot)

                for way in (2, -2, 1, -1):
                    self.pass_on(slot, way)

            loop(4, body)

        def relay_wide(self, low, count):
            def body(i):
                j = i + low
                for way in (1, -1):
                    slot = self.slot(j, -2 * way)
                    self.arrive(slot)
                    self.pass_on(slot, way)

                    @pl.when(rem(j, 2) == (0 if way > 0 else 1))
                    def _():
                        self.pass_on(slot, 2 * way)

            loop(count, body)

        def finish_wide(self):
            def body(j):
                for away in (1, -1, 3, -3, 4):
                    self.arrive(self.slot(j, away))

            loop(8, body)

        def spread_near(self):
            for e in (1, -1, 2, -2):
                there = place(rem(p + e + RING, RING), q)
                remote(self.piece(f), self.piece(f), self.send, self.recv.at[f], fs=there).start()

        def relay(self, slot, e):
            there = place(rem(p + e + RING, RING), q)
            remote(
                self.piece(slot), self.piece(slot), self.send, self.recv.at[slot], fs=there
            ).start()

        def near(self, ways=(1, -1)):
            for j, off in enumerate((0, 1, -1, 2, -2)):
                slot = place(rem(p + off + RING, RING), q)
                if j > 0:
                    self.arrive(slot)
                else:
                    self.share(slot)
                if j > 2:
                    way = 1 if off < 0 else -1
                    self.relay(slot, way)

                    @pl.when(rem(p, 2) == (0 if off < 0 else 1))
                    def _():
                        self.relay(slot, 2 * way)

                for way in ways:
                    self.pass_on(slot, way)

        def late(self, ways=(1, -1)):
            for off in (3, -3, 4):
                slot = place(rem(p + off + RING, RING), q)
                self.arrive(slot)
                for way in ways:
                    self.pass_on(slot, way)

        def hop(self, far, half):
            def body(i):
                j = i + 4 * half
                k = j + 4 if far == 3 else j
                from_left, from_right = self.slot(j, -far), self.slot(k, far)
                self.arrive(from_left)
                self.pass_on(from_left, 1)
                self.arrive(from_right)
                self.pass_on(from_right, -1)

            loop(4, body)

        def hop_last(self, way):
            def body(j):
                slot = self.slot(j if way > 0 else j + 4, -3 * way)
                self.arrive(slot)
                self.pass_on(slot, way)

            loop(4, body)

        def finish(self):
            def body(j):
                self.arrive(self.slot(j + 4, -3))
                self.arrive(self.slot(j, 3))
                self.arrive(self.slot(j, 4))
                self.arrive(self.slot(j + 4, 4))

            loop(4, body)

    ga = Gather(lambda s: a_all.at[s], a_recv, ring_send.at[0])
    def share(slot):
        rows = o_all.at[slot, c]
        remote(rows, rows, swap_send, swap_recv, tp=partner).start()

    go = Gather(lambda s: o_all.at[s, c], o_recv, ring_send.at[1], share)
    gf = Gather(lambda s: f_all.at[s], f_recv, ring_send.at[2])

    loads[0].wait()
    loads[1].wait()
    ga.spread()

    loads[2].wait()
    own_lanes = pl.ds(pl.multiple_of(t * 128, 128), 128)
    for e in range(1, 8):
        other = rem(t + e, 8)
        half = rem(other, 2)
        remote(
            o_own.at[half], o_all.at[f, half, :, own_lanes], pre_send, pre_recv.at[t], tp=other
        ).start()
    own_out = pltpu.make_async_copy(o_own.at[c], o_all.at[f, c, :, own_lanes], load_sem.at[15])
    own_out.start()

    class Rows:
        def __init__(self, ref, recv, send):
            self.ref, self.recv, self.send = ref, recv, send

        def pass_on(self, at, tp):
            remote(self.ref.at[at], self.ref.at[at], self.send, self.recv.at[at], tp=tp).start()

        def arrive(self, at):
            hold(self.ref.at[at], self.recv.at[at])

        def own(self, k):
            at = t * SUBS + k
            self.pass_on(at, 2 * chip(turn) + c)
            self.pass_on(at, 2 * chip(-turn) + c)
            self.pass_on(at, partner)

        def behind(self, k):
            at = (2 * chip(-turn) + c) * SUBS + k
            self.arrive(at)
            self.pass_on(at, 2 * chip(turn) + c)
            self.pass_on(at, partner)

        def ahead(self, k):
            at = (2 * chip(turn) + c) * SUBS + k
            self.arrive(at)
            self.pass_on(at, partner)

        def far(self, k):
            at = (2 * chip(2) + c) * SUBS + k
            self.arrive(at)
            self.pass_on(at, partner)

        def paired(self, chip_at):
            for k in range(SUBS):
                self.arrive((2 * chip_at + 1 - c) * SUBS + k)

        def drain(self):
            hold(self.ref.at[pl.ds(0, 7 * SUBS)], self.send)

        def block(self, tp):
            rows = self.ref[pl.ds(tp * SUBS, SUBS)]
            return rows.reshape(ROWS, D)

    r1 = Rows(n1, n_recv, n_send.at[0])
    r2 = Rows(n2, n_recv, n_send.at[1])

    loop(SUBS, r1.own)

    for i in (4, 5, 6, 12, 13, 14):
        loads[i].wait()
    gf.spread_near()
    ga.first_wide(0)
    ga.first_wide(1)
    own_out.wait()
    for e in range(1, 8):
        other = rem(t + e, 8)
        lanes = pl.ds(pl.multiple_of(other * 128, 128), 128)
        hold(o_all.at[f, c, :, lanes], pre_recv.at[other])
    go.spread_near()
    r1.behind(0)
    r1.ahead(0)
    ga.relay_wide(0, 4)
    ga.relay_wide(4, 4)
    r1.behind(1)
    r1.ahead(1)
    go.near()
    gf.near()
    r1.behind(2)
    r1.ahead(2)
    r1.behind(3)
    r1.ahead(3)
    ga.finish_wide()
    go.late()
    go.hop(1, 0)

    def project(chip_at):
        r1.paired(chip_at)
        rows = n1[pl.ds(2 * chip_at * SUBS, 2 * SUBS)].reshape(2 * ROWS, D)
        both = jnp.dot(rows, a_all[...].reshape(D, 256), preferred_element_type=F32)
        both = both.astype(BF16).astype(F32)
        at = chip_at * 2 * ROWS
        branch[pl.ds(pl.multiple_of(at + 8, 8), 2 * ROWS), :] = both[:, :128]
        gel[pl.ds(pl.multiple_of(at, 8), 2 * ROWS), :] = both[:, 128:]

    r1.far(0)
    r1.far(1)
    project(x)
    r1.far(2)
    project(chip(turn))
    r1.far(3)
    project(chip(-turn))
    go.hop(1, 1)
    project(chip(2))
    go.hop(2, 0)

    taps = conv_weight[...].astype(F32)

    def gate(s):
        window = branch[pl.ds(pl.multiple_of(s * 128, 8), 144), :]
        summed = taps[0:1] * window[6:134]
        for offset in range(1, 4):
            summed = summed + taps[offset : offset + 1] * window[6 + offset : 134 + offset]
        conv = summed.astype(BF16)
        wide = conv.astype(F32)
        both = jnp.dot(conv, gates[...], preferred_element_type=F32)
        at = pl.ds(pl.multiple_of(s * SEG, 8), 128)
        for d, (ret, fee) in enumerate(((ret0, fee0), (ret1, fee1))):
            rate = sigmoid(both[:, 256 * d : 256 * d + 128])
            inflow = sigmoid(both[:, 256 * d + 128 : 256 * d + 256])
            log_retain = rate * scale[pl.ds(d, 1), :]
            retain = jnp.exp(log_retain)
            u = 2.0 * log_retain
            near = 1.0 + u * (0.2 * (1.0 + u * (1.0 / 6.0)))
            near = 1.0 + u * (1.0 / 3.0) * (1.0 + u * 0.25 * near)
            near = -u * (1.0 + 0.5 * u * near)
            lost = jnp.where(u > -0.25, near, 1.0 - retain * retain)
            ret[at, :] = retain
            fee[at, :] = jnp.sqrt(lost) * inflow * wide

    loop(4, gate)
    go.hop(2, 1)
    loop(4, lambda s: gate(s + 4))

    one, zero = jnp.ones((8, 128), F32), jnp.zeros((8, 128), F32)

    def scan(i, carry):
        h0, a0, h1, a1 = carry
        for k in range(8):
            up = pl.ds(i * 8 + k, 8, stride=SEG)
            down = pl.ds(127 - (i * 8 + k), 8, stride=SEG)
            r, v = ret0[up, :], fee0[up, :]
            h0 = r * h0 + v
            a0 = r * a0
            fee0[up, :] = h0
            ret0[up, :] = a0
            r, v = ret1[down, :], fee1[down, :]
            h1 = r * h1 + v
            a1 = r * a1
            fee1[down, :] = h1
            ret1[down, :] = a1
        return h0, a0, h1, a1

    h0, a0, h1, a1 = lax.fori_loop(0, 16, scan, (zero, one, zero, one))
    state = jnp.zeros((1, 128), F32)
    for s in range(8):
        carry_in[s : s + 1, :] = state
        state = a0[s : s + 1] * state + h0[s : s + 1]
    state = jnp.zeros((1, 128), F32)
    for s in reversed(range(8)):
        carry_in[8 + s : 9 + s, :] = state
        state = a1[s : s + 1] * state + h1[s : s + 1]

    def mix(e):
        m = lax.div(e, jnp.int32(2))
        away = jnp.where(m == 3, 0, jnp.where(m == 2, 3, 2 - m))
        s = 2 * chip(away) + rem(c + 1 + e, 2)
        at = pl.ds(pl.multiple_of(s * SEG, 8), 128)
        state = fee0[at, :] + ret0[at, :] * carry_in[pl.ds(s, 1), :]
        state = state + (fee1[at, :] + ret1[at, :] * carry_in[pl.ds(8 + s, 1), :])
        value = gelu(gel[pl.ds(pl.multiple_of(s * 128, 8), 128), :]) * state
        mixed[s] = value.astype(BF16)

        @pl.when(e < 7)
        def _():
            remote(mixed.at[s], hidden.at[t], mix_send, mix_recv.at[t], tp=s).start()

        @pl.when(e == 7)
        def _():
            hidden[s] = value.astype(BF16)

    loop(8, mix)
    go.hop(3, 0)
    gf.late()
    gf.hop(1, 0)
    go.finish()
    for e in range(1, 8):
        other = rem(t + e, 8)
        hold(hidden.at[other], mix_recv.at[other])

    wide_hidden = jnp.concatenate([hidden[i] for i in range(8)], axis=1)

    hold(o_all.at[:, 1 - c], swap_recv)

    def project_out(part):
        weight = o_all[pl.ds(16 * part, 16)].reshape(512, 1024)
        msum[:, pl.ds(pl.multiple_of(part * 512, 128), 512)] = lax.dot_general(
            wide_hidden, weight, NT, preferred_element_type=F32
        )

    loop(4, project_out)

    def norm_mid(k):
        for h in range(SUB // 16):
            at = pl.ds(pl.multiple_of(k * SUB + 16 * h, 16), 16)
            total = tok[at, :].astype(F32) + normed(msum[at, :], post_mix[...])
            total = total.astype(BF16)
            res[at, :] = total
            n2[t * SUBS + k, pl.ds(16 * h, 16), :] = normed(
                total.astype(F32), pre_ffn[...]
            ).astype(BF16)
        r2.own(k)

    loop(SUBS, norm_mid)
    gf.hop(1, 1)
    gf.hop(2, 0)
    r2.behind(0)
    r2.ahead(0)
    gf.hop(2, 1)
    r2.behind(1)
    r2.ahead(1)
    gf.hop_last(1)
    r2.behind(2)
    r2.ahead(2)
    gf.hop_last(-1)
    r2.behind(3)
    r2.ahead(3)
    gf.finish()

    def feed_up(i):
        away = 2 if i == 0 else 0 if i == 3 else -turn if i == 1 else turn
        mine = chip(away)
        theirs = chip(-away)
        r2.paired(theirs)
        rows = jnp.concatenate([r2.block(2 * theirs + 1 - c), r2.block(2 * mine + c)], axis=0)
        for n in range(3):
            gu[:, pl.ds(256 * n, 256)] = jnp.dot(
                rows, f_all[:, :, pl.ds(256 * n, 256)].reshape(D, 256), preferred_element_type=F32
            )
        for h in range(4):
            at = pl.ds(64 * h, 64)
            g = gu[at, pl.ds(0, 384)]
            hid[at, :] = (g * sigmoid(g) * gu[at, pl.ds(384, 384)]).astype(BF16)

    def feed_down(i):
        def down(n):
            weight = f_all[pl.ds(16 * n, 16), :, pl.ds(768, 384)].reshape(512, 384)
            part = lax.dot_general(hid[...], weight, NT, preferred_element_type=F32)
            give[i, n] = part[:ROWS].astype(BF16)
            keep[i, n] = part[ROWS:]
            remote(
                give.at[i, n], got.at[i, n], pair_send, pair_recv.at[i, n], tp=partner
            ).start()

        loop(4, down)

    def pass_sum(o, low, count):
        target = 2 * chip(-turn if o == 1 else turn) + c

        def add(m):
            n = m + low
            hold(got.at[o, n], pair_recv.at[o, n])
            if o == 2:
                hold(land.at[0, n], land_recv.at[0, n])
            for h in range(ROWS // SUB):
                at = pl.ds(SUB * h, SUB)
                total = keep[o, n, at, :] + got[o, n, at, :].astype(F32)
                if o == 2:
                    total = total + land[0, n, at, :].astype(F32)
                sums[o, n, at, :] = total.astype(BF16)
            remote(
                sums.at[o, n], land.at[o, n], land_send, land_recv.at[o, n], tp=target
            ).start()

        loop(count, add)

    feed_up(1)
    feed_down(1)
    for k in range(SUBS):
        r2.far(k)
    pass_sum(1, 0, 2)
    feed_up(2)
    pass_sum(1, 2, 2)
    feed_down(2)
    feed_up(0)
    feed_down(0)
    pass_sum(0, 0, 2)
    feed_up(3)
    pass_sum(0, 2, 2)
    feed_down(3)
    pass_sum(2, 0, 4)

    power[...] = jnp.zeros_like(power)

    def own_sum(n):
        hold(got.at[3, n], pair_recv.at[3, n])
        hold(land.at[1, n], land_recv.at[1, n])
        hold(land.at[2, n], land_recv.at[2, n])
        for h in range(ROWS // SUB):
            at = pl.ds(SUB * h, SUB)
            total = keep[3, n, at, :] + got[3, n, at, :].astype(F32)
            total = total + land[1, n, at, :].astype(F32)
            total = total + land[2, n, at, :].astype(F32)
            keep[3, n, at, :] = total
            square = total * total
            square = square[:, :256] + square[:, 256:]
            power[at, :] += square[:, :128] + square[:, 128:]

    loop(4, own_sum)

    def last(k):
        for h in range(SUB // 16):
            at = pl.ds(pl.multiple_of(k * SUB + 16 * h, 16), 16)
            mean = jnp.sum(power[at, :], axis=-1, keepdims=True) * (1.0 / D)
            factor = lax.rsqrt(mean + EPS)
            for n in range(4):
                lanes = pl.ds(512 * n, 512)
                value = keep[3, n, at, :] * factor * post_ffn[:, lanes]
                final_rows[at, lanes] = (res[at, lanes].astype(F32) + value).astype(BF16)
        rows = pl.ds(pl.multiple_of(k * SUB, SUB), SUB)
        pltpu.make_async_copy(final_rows.at[rows], out.at[rows], load_sem.at[k]).start()

    loop(SUBS, last)

    for k in range(SUBS):
        hold(final_rows.at[pl.ds(0, SUB)], load_sem.at[k])
    hold(a_all.at[pl.ds(0, 63)], ring_send.at[0])
    hold(o_all.at[pl.ds(0, 63), 0], ring_send.at[1])
    hold(f_all.at[pl.ds(0, 63)], ring_send.at[2])
    hold(o_all.at[0, 0, :, pl.ds(0, 896)], pre_send)
    hold(o_all.at[:, c], swap_send)
    r1.drain()
    r2.drain()
    hold(mixed.at[pl.ds(0, 7)], mix_send)
    hold(give, pair_send)
    hold(sums, land_send)


def per_device(
    tokens,
    pre_mix_gain,
    post_mix_gain,
    pre_ffn_gain,
    post_ffn_gain,
    w_branch,
    w_gelu,
    conv_weight,
    w_rec,
    w_inp,
    decay,
    out_weight_t,
    w_gate,
    w_up,
    down_weight_t,
):
    gains = [
        g.reshape(1, D) for g in (pre_mix_gain, post_mix_gain, pre_ffn_gain, post_ffn_gain)
    ]
    far = pl.BlockSpec(memory_space=pltpu.HBM)
    dma = pltpu.SemaphoreType.DMA
    return pl.pallas_call(
        layer,
        out_shape=jax.ShapeDtypeStruct((ROWS, D), BF16),
        in_specs=[far] * 15,
        out_specs=far,
        scratch_shapes=[
            pltpu.VMEM((1, D), F32),
            pltpu.VMEM((1, D), F32),
            pltpu.VMEM((1, D), F32),
            pltpu.VMEM((1, D), F32),
            pltpu.VMEM((4, 128), BF16),
            pltpu.VMEM((2, 1, 128, 128), BF16),
            pltpu.VMEM((2, 1, 128, 128), BF16),
            pltpu.VMEM((2, 128), F32),
            pltpu.VMEM((ROWS, D), BF16),
            pltpu.VMEM((8 * SUBS, SUB, D), BF16),
            pltpu.VMEM((8 * SUBS, SUB, D), BF16),
            pltpu.VMEM((64, 32, 256), BF16),
            pltpu.VMEM((64, 2, 16, 1024), BF16),
            pltpu.VMEM((64, 32, 1152), BF16),
            pltpu.VMEM((2, 16, 128), BF16),
            pltpu.VMEM((1040, 128), F32),
            pltpu.VMEM((1024, 128), F32),
            pltpu.VMEM((8 * SEG, 128), F32),
            pltpu.VMEM((8 * SEG, 128), F32),
            pltpu.VMEM((8 * SEG, 128), F32),
            pltpu.VMEM((8 * SEG, 128), F32),
            pltpu.VMEM((128, 512), BF16),
            pltpu.VMEM((2, 128), F32),
            pltpu.VMEM((16, 128), F32),
            pltpu.VMEM((8, 128, 128), BF16),
            pltpu.VMEM((8, 128, 128), BF16),
            pltpu.VMEM((ROWS, D), F32),
            pltpu.VMEM((ROWS, D), BF16),
            pltpu.VMEM((2 * ROWS, 768), F32),
            pltpu.VMEM((2 * ROWS, 384), BF16),
            pltpu.VMEM((4, 4, ROWS, 512), F32),
            pltpu.VMEM((4, 4, ROWS, 512), BF16),
            pltpu.VMEM((4, 4, ROWS, 512), BF16),
            pltpu.VMEM((3, 4, ROWS, 512), BF16),
            pltpu.VMEM((3, 4, ROWS, 512), BF16),
            pltpu.VMEM((ROWS, 128), F32),
            pltpu.VMEM((ROWS, D), BF16),
            dma((16,)),
            dma((64,)),
            dma((64,)),
            dma((64,)),
            dma((3,)),
            dma((8,)),
            dma,
            dma,
            dma,
            dma((8 * SUBS,)),
            dma((2,)),
            dma((8,)),
            dma,
            dma((4, 4)),
            dma,
            dma((3, 4)),
            dma,
        ],
        compiler_params=pltpu.CompilerParams(
            collective_id=0, has_side_effects=True, vmem_limit_bytes=60 * 1024 * 1024
        ),
    )(
        tokens,
        *gains,
        w_branch,
        w_gelu,
        conv_weight,
        w_rec,
        w_inp,
        decay,
        out_weight_t.reshape(2, 16, 128),
        w_gate,
        w_up,
        down_weight_t,
    )


def solution(mesh):
    return jax.shard_map(
        per_device,
        mesh=mesh,
        in_specs=(
            P(("fs", "tp"), None),
            P(),
            P(),
            P(),
            P(),
            P("fs", "tp"),
            P("fs", "tp"),
            P(None, "tp"),
            P(None, "tp", None, None),
            P(None, "tp", None, None),
            P(None, "tp"),
            P("fs", "tp"),
            P("fs", "tp"),
            P("fs", "tp"),
            P("fs", "tp"),
        ),
        out_specs=P(("fs", "tp"), None),
        check_vma=False,
    )
```
